128 devices in a mesh: sp: 16 (over z, y), dp: 8 (over x, core).
Axes of the slice: x: 4, y: 4, z: 4, core: 2. Of those that a mesh axis runs over, the one named last changes fastest.
Arguments:
- u_pre: bfloat16 [8, 16384, 2048], P('dp', 'sp'), may hold values from -6 to 6
- v_pre: bfloat16 [8, 16384, 2048], P('dp', 'sp'), may hold values from -6 to 6
- d_out: bfloat16 [8, 16384, 2048], P('dp', 'sp'), may hold values from -6 to 6
- w_mix: bfloat16 [16, 128, 128], replicated, may hold values from -0.5 to 0.5
- mix_bias: float32 [16, 128], replicated, may hold values from 0.1 to 1.9
- norm_gain: float32 [16, 128], replicated, may hold values from 0.1 to 1.9
- norm_shift: float32 [16, 128], replicated, may hold values from -3 to 3
- w_out: bfloat16 [2048, 2048], P('dp'), may hold values from -0.125 to 0.125
Outputs:
- grad_u: bfloat16 [8, 16384, 2048], P('dp', 'sp')
- grad_v: bfloat16 [8, 16384, 2048], P('dp', 'sp')
- grad_w_out: float32 [2048, 2048], P('dp')
- grad_w_mix: float32 [16, 128, 128], replicated
- grad_mix_bias: float32 [16, 128], replicated
- grad_gain: float32 [16, 128], replicated
- grad_shift: float32 [16, 128], replicated
The draws below stay inside these ranges and needn't reach their ends.
All inputs are finite; a program needn't handle non-finite values.
Results may differ from the reference program's by a relative error of at most 0.012.
Values may be sent and summed in bfloat16 or wider, within the bound.
No kernel may reach another device: no remote copies, remote signals or barrier semaphores. Data moves between devices by JAX's collectives and lax.ppermute only.
A program may use at most 192 MiB of HBM per device.

```python
import jax
import jax.numpy as jnp
from jax import lax

D = 2048
GROUPS = 16
CHANS = 128
BLOCK = 128
SGU_W = 2048
SEQLEN = 16384
SEQS = 8


def block_scale(stream_key, extent, shards, least, largest):
    def one(axis_at, blocks):
        heights = jax.random.uniform(jax.random.fold_in(jax.random.fold_in(stream_key, 6), axis_at), (blocks,), jnp.float32, least / len(shards), largest / len(shards))
        return jnp.repeat(jnp.exp(heights), extent[axis_at] // blocks).reshape((-1,) + (1,) * (len(extent) - axis_at - 1))

    factor_of = one(*shards[0])
    for cut in shards[1:]:
        factor_of = factor_of * one(*cut)
    return factor_of


def scatter_about(stream_key, shape, spread, bound, split=(), kind=jnp.bfloat16):
    entries = jax.random.normal(stream_key, shape, jnp.float32) * spread
    if len(split) > 0:
        entries = block_scale(stream_key, shape, split, -0.22, 0.18) * entries
    return jnp.clip(entries, min=-bound, max=bound).astype(kind)


def setup_inputs(seed: int = 0) -> dict:
    arg_keys = jax.random.split(jax.random.key(seed), 9)
    u_pre = scatter_about(arg_keys[0], (SEQS, SEQLEN, SGU_W), 1.0, 6.0, ((0, 8), (1, 16)))
    v_pre = scatter_about(arg_keys[1], (SEQS, SEQLEN, SGU_W), 1.0, 6.0, ((0, 8), (1, 16)))
    d_out = scatter_about(arg_keys[2], (SEQS, SEQLEN, D), 1.0, 6.0, ((0, 8), (1, 16)))
    w_mix = scatter_about(arg_keys[3], (GROUPS, BLOCK, BLOCK), BLOCK ** -0.5, 0.5)
    mix_bias = jnp.clip(1.0 + 0.18 * jax.random.normal(arg_keys[4], (GROUPS, BLOCK), jnp.float32), 0.1, 1.9)
    norm_gain = jnp.clip(1.0 + 0.18 * jax.random.normal(arg_keys[5], (GROUPS, CHANS), jnp.float32), 0.1, 1.9)
    norm_shift = scatter_about(arg_keys[6], (GROUPS, CHANS), 0.5, 3.0, (), jnp.float32)
    w_out = scatter_about(arg_keys[7], (SGU_W, D), SGU_W ** -0.5, 0.125, ((0, 8),))
    return {"u_pre": u_pre, "v_pre": v_pre, "d_out": d_out, "w_mix": w_mix, "mix_bias": mix_bias, "norm_gain": norm_gain, "norm_shift": norm_shift, "w_out": w_out}


EPS = 1e-05

def mechanism(grad_s, u_pre, v_pre, w_mix, mix_bias, gain, shift):
    items, length, width = grad_s.shape
    groups, span = (w_mix.shape[0], w_mix.shape[1])
    chans = width // groups
    shape = (items, length // span, span, groups, chans)
    u_val = u_pre.astype(jnp.float32).reshape(shape)
    v_val = v_pre.astype(jnp.float32).reshape(shape)
    cotan = grad_s.astype(jnp.float32).reshape(shape)
    upper, u_back = jax.vjp(jax.nn.gelu, u_val)
    gated, v_back = jax.vjp(jax.nn.gelu, v_val)
    centre = gated - lax.optimization_barrier(jnp.mean(gated, axis=-1, keepdims=True))
    inverse = lax.rsqrt(lax.optimization_barrier(jnp.mean(centre * centre, axis=-1, keepdims=True)) + EPS)
    scaled = centre * inverse
    normed = (scaled * gain + shift).astype(jnp.bfloat16)
    lower = jnp.tril(jnp.ones((span, span), dtype=bool))
    w_low = jnp.where(lower[None], w_mix, jnp.zeros_like(w_mix))
    mixed = jnp.einsum('gts,insgc->intgc', w_low.astype(jnp.float32), normed.astype(jnp.float32))
    mixed = mixed + jnp.transpose(mix_bias)[:, :, None]
    gated_out = (upper * mixed).astype(jnp.bfloat16)
    d_mixed = cotan * upper
    d_mixed_b = d_mixed.astype(jnp.bfloat16)
    grad_u = u_back(cotan * mixed)[0].astype(jnp.bfloat16).reshape(items, length, width)
    grad_bias = jnp.transpose(lax.optimization_barrier(jnp.sum(d_mixed, axis=(0, 1, 4))))
    grad_w = jnp.einsum('intgc,insgc->gts', d_mixed_b.astype(jnp.float32), normed.astype(jnp.float32))
    grad_w = jnp.where(lower[None], grad_w, jnp.zeros_like(grad_w))
    d_normed = jnp.einsum('gts,intgc->insgc', w_low.astype(jnp.float32), d_mixed_b.astype(jnp.float32))
    grad_gain = lax.optimization_barrier(jnp.sum(d_normed * scaled, axis=(0, 1, 2)))
    grad_shift = lax.optimization_barrier(jnp.sum(d_normed, axis=(0, 1, 2)))
    d_scaled = d_normed * gain
    d_gated = inverse * (d_scaled - lax.optimization_barrier(jnp.mean(d_scaled, axis=-1, keepdims=True)) - scaled * lax.optimization_barrier(jnp.mean(d_scaled * scaled, axis=-1, keepdims=True)))
    grad_v = v_back(d_gated)[0].astype(jnp.bfloat16).reshape(items, length, width)
    return (grad_u, grad_v, gated_out.reshape(items, length, width), grad_w, grad_bias, grad_gain, grad_shift)

def reference(u_pre, v_pre, d_out, w_mix, mix_bias, norm_gain, norm_shift, w_out):
    flat_d = d_out.reshape(-1, D)
    grad_s = jnp.dot(flat_d, jnp.transpose(w_out), preferred_element_type=jnp.float32)
    grad_s = grad_s.astype(jnp.bfloat16).reshape(SEQS, SEQLEN, SGU_W)

    def one_sequence(packed):
        cot, upre, vpre = packed
        return mechanism(cot[None], upre[None], vpre[None], w_mix, mix_bias, norm_gain, norm_shift)
    grad_u, grad_v, gated_out, grad_w, grad_bias, grad_gain, grad_shift = lax.map(one_sequence, (grad_s, u_pre, v_pre))
    grad_u = grad_u.reshape(SEQS, SEQLEN, SGU_W)
    grad_v = grad_v.reshape(SEQS, SEQLEN, SGU_W)
    flat_s = gated_out.reshape(-1, SGU_W)
    grad_w_out = jnp.dot(jnp.transpose(flat_s), flat_d, preferred_element_type=jnp.float32)
    return (grad_u, grad_v, grad_w_out, lax.optimization_barrier(jnp.sum(grad_w, axis=0)), lax.optimization_barrier(jnp.sum(grad_bias, axis=0)), lax.optimization_barrier(jnp.sum(grad_gain, axis=0)), lax.optimization_barrier(jnp.sum(grad_shift, axis=0)))
```

```python
import functools

import jax
import jax.numpy as jnp
from jax import lax
from jax.experimental import pallas as pl
from jax.experimental.pallas import tpu as pltpu
from jax.sharding import Mesh, PartitionSpec as P

EPS = 1e-05
C0 = 0.7978845608028654
C1 = C0 * 0.044715
F32 = jnp.float32
BF16 = jnp.bfloat16
BLK = 128
PAIR = 256
CHUNK = 24
ROOT = BLK**0.5


def tanh_of(a):
    a2 = a * a
    return jnp.tanh(a * (C0 + C1 * a2)), a2


def gelu(a):
    t, _ = tanh_of(a)
    return a * (0.5 + 0.5 * t)


def gelu_and_slope(a):
    t, a2 = tanh_of(a)
    half = 0.5 + 0.5 * t
    value = a * half
    return value, half + value * (1.0 - half) * (2.0 * C0 + (6.0 * C1) * a2)


def norm(gated):
    centre = gated - jnp.mean(gated, axis=-1, keepdims=True)
    inverse = lax.rsqrt(jnp.sum(centre * centre, axis=-1, keepdims=True) + BLK * EPS)
    return centre * inverse, inverse


def columns(ref, at, first=0, count=None):
    count = ref.shape[0] if count is None else count
    return jnp.concatenate([ref[first + k, at] for k in range(count)], axis=1)


def scatter_columns(src, dst, sem):
    @pl.loop(0, dst.shape[0])
    def _(k):
        at = pl.ds(pl.multiple_of(k * BLK, BLK), BLK)
        pltpu.make_async_copy(src.at[:, at], dst.at[k], sem).start()


def await_all(dst, sem):
    pltpu.make_async_copy(dst, dst, sem).wait()


def cols_of(g):
    return slice(g * BLK, (g + 1) * BLK)


def forward_kernel(
    order, u_ref, v_ref, d_hbm, w_ref, bias_ref, gain_ref, shift_ref, out_ref, d_ref, go_ref, bias_at, sem
):
    blocks, length, _ = d_ref.shape
    turns = length // PAIR
    step = pl.program_id(0)
    last = pl.num_programs(0) - 1
    now, before = lax.rem(step, 2), lax.rem(step + 1, 2)
    part = blocks // turns

    def multiply(i):
        out_ref[0, :, i * part * BLK : (i + 1) * part * BLK] = jnp.dot(
            go_ref[before],
            columns(d_ref, slice(None), i * part, part),
            preferred_element_type=F32,
        ).astype(out_ref.dtype)

    def gate(i):
        rows = [slice(i * PAIR + h * BLK, i * PAIR + (h + 1) * BLK) for h in range(2)]
        for g in range(2):
            gain, shift = ROOT * gain_ref[0, g : g + 1], shift_ref[0, g : g + 1]
            normed = []
            for at in rows:
                scaled, _ = norm(gelu(v_ref[at, cols_of(g)].astype(F32)))
                normed.append((scaled * gain + shift).astype(BF16))
            mixed = jnp.dot(
                w_ref[0, g], jnp.concatenate(normed, axis=1), preferred_element_type=F32
            )
            for h, at in enumerate(rows):
                upper = gelu(u_ref[at, cols_of(g)].astype(F32))
                gated_out = (upper * (mixed[:, cols_of(h)] + bias_at[g])).astype(BF16)
                go_ref[now, cols_of(g), at] = gated_out.T

    @pl.when(step == 0)
    def _():
        scatter_columns(d_hbm, d_ref, sem)

    for g in range(2):
        bias_at[g] = jnp.broadcast_to(bias_ref[0, :, g : g + 1], (BLK, BLK))

    @pl.when(step == 0)
    def _():
        for i in range(turns):
            gate(i)
        await_all(d_ref, sem)

    @pl.when((step > 0) & (step < last))
    def _():
        for i in range(turns):
            multiply(i)
            gate(i)

    @pl.when(step == last)
    def _():
        for i in range(turns):
            multiply(i)


def forward(order, u, v, d, w_low, bias, gain, shift):
    n = order.shape[0]
    length, width = u.shape
    last = n - 1
    cur = lambda j, o: (0, o[jnp.minimum(j, last)])
    par = lambda j, o: (o[jnp.minimum(j, last)], 0, 0)
    return pl.pallas_call(
        forward_kernel,
        grid_spec=pltpu.PrefetchScalarGridSpec(
            num_scalar_prefetch=1,
            grid=(n + 1,),
            in_specs=[
                pl.BlockSpec((length, PAIR), cur),
                pl.BlockSpec((length, PAIR), cur),
                pl.BlockSpec(memory_space=pl.ANY),
                pl.BlockSpec((1, 2, BLK, BLK), lambda j, o: (o[jnp.minimum(j, last)], 0, 0, 0)),
                pl.BlockSpec((1, BLK, 2), par),
                pl.BlockSpec((1, 2, BLK), par),
                pl.BlockSpec((1, 2, BLK), par),
            ],
            out_specs=pl.BlockSpec((1, PAIR, width), lambda j, o: (jnp.maximum(j - 1, 0), 0, 0)),
            scratch_shapes=[
                pltpu.VMEM((width // BLK, length, BLK), BF16),
                pltpu.VMEM((2, PAIR, length), BF16),
                pltpu.VMEM((2, BLK, BLK), F32),
                pltpu.SemaphoreType.DMA,
            ],
        ),
        out_shape=jax.ShapeDtypeStruct((n, PAIR, width), BF16),
        cost_estimate=pl.CostEstimate(
            flops=2 * n * PAIR * length * (width + BLK) * 2,
            bytes_accessed=length * width * 2 + n * PAIR * (4 * length + 2 * width),
            transcendentals=2 * n * PAIR * length,
        ),
        name="fwd",
    )(order, u, v, d, w_low, bias, gain, shift)


def backward_kernel(
    pieces, order, u_ref, v_ref, d_hbm, low_ref, lowt_ref, bias_ref, gain_ref, shift_ref, *rest
):
    count = len(pieces)
    w_hbm = rest[:count]
    gu_ref, gv_ref, pack_ref = rest[-12:-9]
    d_ref, w_ref, cot_ref, bias_at, b_acc, g_acc, s_acc, m_acc, sems = rest[-9:]
    turns = u_ref.shape[0] // PAIR
    step = pl.program_id(0)
    last = pl.num_programs(0) - 1

    def landing(k):
        slot, start, size = pieces[k]
        return w_ref.at[slot, :, pl.ds(start, size)]

    def cotangent(i, slot):
        return lax.dot_general(
            columns(d_ref, slice(i * PAIR, (i + 1) * PAIR)),
            columns(w_ref.at[slot], slice(None)),
            (((1,), (1,)), ((), ())),
            preferred_element_type=F32,
        )

    @pl.when(step == 0)
    def _():
        for k in range(count):
            if pieces[k][0] == 0:
                scatter_columns(w_hbm[k], landing(k), sems.at[k])
        scatter_columns(d_hbm, d_ref, sems.at[count])
        for k in range(count):
            if pieces[k][0] > 0:
                scatter_columns(w_hbm[k], landing(k), sems.at[k])
        for k in range(count):
            if pieces[k][0] == 0:
                await_all(landing(k), sems.at[k])
        await_all(d_ref, sems.at[count])
        cot_ref[0] = cotangent(0, 0)

    for k in range(count):
        if pieces[k][0] > 0:
            @pl.when(step == pieces[k][0] - 1)
            def _(k=k):
                await_all(landing(k), sems.at[k])

    for g in range(2):
        bias_at[g] = jnp.broadcast_to(bias_ref[0, :, g : g + 1], (BLK, BLK))
    b_acc[...] = jnp.zeros_like(b_acc)
    g_acc[...] = jnp.zeros_like(g_acc)
    s_acc[...] = jnp.zeros_like(s_acc)
    m_acc[...] = jnp.zeros_like(m_acc)
    for i in range(turns):
        if i + 1 < turns:
            cot_ref[(i + 1) % 2] = cotangent(i + 1, step)
        else:
            cot_ref[0] = cotangent(0, jnp.minimum(step + 1, last))
        for g in range(2):
            gain, shift = ROOT * gain_ref[0, g : g + 1], shift_ref[0, g : g + 1]
            rows = [slice(i * PAIR + h * BLK, i * PAIR + (h + 1) * BLK) for h in range(2)]
            kept, normed = [], []
            for at in rows:
                gated, slope = gelu_and_slope(v_ref[at, cols_of(g)].astype(F32))
                scaled, inverse = norm(gated)
                kept.append((scaled, inverse * slope))
                normed.append((scaled * gain + shift).astype(BF16))
            normed = jnp.concatenate(normed, axis=1)
            mixed = jnp.dot(low_ref[0, g], normed, preferred_element_type=F32)
            d_mixed_b = []
            for h, at in enumerate(rows):
                upper, slope = gelu_and_slope(u_ref[at, cols_of(g)].astype(F32))
                cot = cot_ref[i % 2, h * BLK : (h + 1) * BLK, cols_of(g)]
                d_mixed = cot * upper
                d_mixed_b.append(d_mixed.astype(BF16))
                b_acc[g] += d_mixed
                gu_ref[at, cols_of(g)] = (
                    cot * slope * (mixed[:, cols_of(h)] + bias_at[g])
                ).astype(BF16)
            d_mixed_b = jnp.concatenate(d_mixed_b, axis=1)
            m_acc[g] += lax.dot_general(
                d_mixed_b, normed, (((1,), (1,)), ((), ())), preferred_element_type=F32
            )
            d_normed = jnp.dot(lowt_ref[0, g], d_mixed_b, preferred_element_type=F32)
            for h, at in enumerate(rows):
                scaled, scale = kept[h]
                dn = d_normed[:, cols_of(h)]
                weighted = dn * scaled
                g_acc[g] += jnp.sum(weighted.reshape(BLK // 8, 8, BLK), axis=0)
                s_acc[g] += jnp.sum(dn.reshape(BLK // 8, 8, BLK), axis=0)
                e = dn * gain
                mean_e = jnp.mean(e, axis=-1, keepdims=True)
                sum_es = jnp.sum(weighted * gain, axis=-1, keepdims=True)
                gv_ref[at, cols_of(g)] = (scale * (e - mean_e - scaled * sum_es)).astype(BF16)

    row = lax.broadcasted_iota(jnp.int32, (BLK, BLK), 0)
    col = lax.broadcasted_iota(jnp.int32, (BLK, BLK), 1)
    filler = jnp.zeros((CHUNK - 17, BLK), F32)
    extra = []
    for g in range(2):
        extra.append(jnp.sum(b_acc[g].T, axis=0, keepdims=True))
        extra.append(ROOT * jnp.sum(g_acc[g], axis=0, keepdims=True))
        extra.append(jnp.sum(s_acc[g], axis=0, keepdims=True))
    for g in range(2):
        lower = jnp.where(row >= col, m_acc[g], 0.0)
        for r in range(8):
            k = g * 8 + r
            vector = extra[k] if k < len(extra) else jnp.zeros((1, BLK), F32)
            pack_ref[0, k] = jnp.concatenate(
                [lower[r * 16 : (r + 1) * 16], vector, filler], axis=0
            ).astype(BF16)


def backward(order, weights, u, v, d, w_low, w_low_t, bias, gain, shift, earlier):
    n = order.shape[0]
    length, width = u.shape
    pairs = width // PAIR
    pieces = tuple((slot, start, w.shape[0]) for slot, start, w in weights)
    cur = lambda j, o: (0, o[j])
    par = lambda j, o: (o[j], 0, 0)
    mat = pl.BlockSpec((1, 2, BLK, BLK), lambda j, o: (o[j], 0, 0, 0))
    tile = pl.BlockSpec((length, PAIR), cur)
    vec = pl.BlockSpec((1, 2, BLK), par)
    col = pl.BlockSpec((1, BLK, 2), par)
    hbm = pl.BlockSpec(memory_space=pl.ANY)
    shapes = [
        jax.ShapeDtypeStruct((length, width), BF16),
        jax.ShapeDtypeStruct((length, width), BF16),
        jax.ShapeDtypeStruct((pairs, 16, CHUNK, BLK), BF16),
    ]
    first = 9 + len(weights)
    alias = {first + k: k for k in range(len(earlier))}
    return pl.pallas_call(
        functools.partial(backward_kernel, pieces),
        grid_spec=pltpu.PrefetchScalarGridSpec(
            num_scalar_prefetch=1,
            grid=(n,),
            in_specs=[
                tile,
                tile,
                hbm,
                mat,
                mat,
                col,
                vec,
                vec,
                *[hbm] * len(weights),
                *[hbm] * len(earlier),
            ],
            out_specs=[
                tile,
                tile,
                pl.BlockSpec((1, 16, CHUNK, BLK), lambda j, o: (o[j], 0, 0, 0)),
            ],
            scratch_shapes=[
                pltpu.VMEM((width // BLK, length, BLK), BF16),
                pltpu.VMEM((n, width // BLK, PAIR, BLK), BF16),
                pltpu.VMEM((2, PAIR, PAIR), F32),
                pltpu.VMEM((2, BLK, BLK), F32),
                pltpu.VMEM((2, BLK, BLK), F32),
                pltpu.VMEM((2, 8, BLK), F32),
                pltpu.VMEM((2, 8, BLK), F32),
                pltpu.VMEM((2, BLK, BLK), F32),
                pltpu.SemaphoreType.DMA((len(weights) + 1,)),
            ],
        ),
        out_shape=shapes,
        input_output_aliases=alias,
        cost_estimate=pl.CostEstimate(
            flops=2 * n * PAIR * length * (width + 3 * BLK) * 2,
            bytes_accessed=length * width * 2 + n * PAIR * (8 * length + 2 * width),
            transcendentals=3 * n * PAIR * length,
        ),
        name="bwd",
    )(order, u, v, d, w_low, w_low_t, bias, gain, shift, *[w for _, _, w in weights], *earlier)


def hop(a, axis, size, by):
    return lax.ppermute(a, axis, [(i, (i + by) % size) for i in range(size)])


def added(a):
    return lax.optimization_barrier(jnp.sum(a.astype(F32), axis=0)).astype(BF16)


def spread(a, axes, count):
    return lax.all_to_all(jnp.broadcast_to(a[None], (count,) + a.shape), axes, 0, 0)


def on_device(u_pre, v_pre, d_out, w_mix, mix_bias, norm_gain, norm_shift, w_out, sizes=None):
    return everything(
        u_pre, v_pre, d_out, w_mix, mix_bias, norm_gain, norm_shift, w_out, sizes
    )


def everything(u_pre, v_pre, d_out, w_mix, mix_bias, norm_gain, norm_shift, w_out, sizes):
    nz, ny, nx, nc = sizes
    plane = nz * ny
    u, v, d = u_pre[0], v_pre[0], d_out[0]
    _, width = u.shape
    groups = w_mix.shape[0]
    pairs = groups // 2
    x, c = lax.axis_index("x"), lax.axis_index("c")
    xs = jnp.arange(nx, dtype=jnp.int32)

    swap = lambda a: hop(a, "c", nc, 1)
    half = w_out.shape[0] // 2
    own = swap(w_out)
    left = hop(w_out, "x", nx, 1)
    right = hop(w_out, "x", nx, -1)
    far0 = hop(left[:half], "x", nx, 1)
    far1 = hop(right[half:], "x", nx, -1)
    near = [swap(left), swap(right)]
    far = [swap(far0), swap(far1)]

    w_low = jnp.tril(w_mix)
    w_low_t = jnp.swapaxes(w_low, 1, 2).reshape(pairs, 2, BLK, BLK)
    w_low = w_low.reshape(pairs, 2, BLK, BLK)
    bias = jnp.swapaxes(mix_bias.reshape(pairs, 2, BLK), 1, 2)
    gain = norm_gain.reshape(pairs, 2, BLK)
    shift = norm_shift.reshape(pairs, 2, BLK)

    common = (u, v, d, w_low, bias, gain, shift)
    theirs = forward(xs * nc + (1 - c), *common)
    ours = forward(xs * nc + c, *common)
    traded = swap(theirs)
    joined = (ours.astype(F32) + traded.astype(F32)).astype(BF16)
    split = lax.all_to_all(joined.reshape(nx * plane, PAIR // plane, width), ("x", "z", "y"), 0, 0)

    backs = (u, v, d, w_low, w_low_t, bias, gain, shift)
    place = lambda k, core: lax.rem(x + k, nx) * nc + core
    order = jnp.stack([place(0, c), place(0, 1 - c)])
    out = backward(order, [(0, 0, w_out), (1, 0, own)], *backs, ())
    order = jnp.stack([place(3, c), place(1, c), place(3, 1 - c), place(1, 1 - c)])
    out = backward(
        order, [(0, 0, left), (1, 0, right), (2, 0, near[0]), (3, 0, near[1])], *backs, out
    )
    order = jnp.stack([place(2, c), place(2, 1 - c)])
    out = backward(
        order, [(0, 0, far0), (0, half, far1), (1, 0, far[0]), (1, half, far[1])], *backs, out
    )
    grad_u, grad_v, packed = out
    packed, split = lax.optimization_barrier((packed, split))
    grad_w_out = spread(added(split), ("z", "y"), plane)
    grad_w_out = grad_w_out.reshape(PAIR, width).astype(F32)
    devices = nz * ny * nx * nc
    every = ("z", "y", "x", "c")
    packed = lax.all_to_all(packed.reshape(devices, CHUNK, BLK), every, 0, 0)
    total = spread(added(packed), every, devices)
    grad_w = total[:, :16].astype(F32).reshape(groups, BLK, BLK)
    rest = total.reshape(pairs, 16, CHUNK, BLK)[:, :6, 16].astype(F32).reshape(groups, 3, BLK)
    vectors = [rest[:, k] for k in range(3)]
    return (grad_u[None], grad_v[None], grad_w_out, grad_w, *vectors)


def solution(mesh):
    devices = mesh.devices.reshape(4, -1, *[mesh.devices.shape[1] // 2, 2])
    grid = Mesh(devices, ("z", "y", "x", "c"))
    big = P(("x", "c"), ("z", "y"), None)
    rows = P(("x", "c"), None)
    return jax.shard_map(
        functools.partial(on_device, sizes=devices.shape),
        mesh=grid,
        in_specs=(big, big, big, P(), P(), P(), P(), rows),
        out_specs=(big, big, rows, P(), P(), P(), P()),
        check_vma=False,
    )
```

```python
import functools

import jax
import jax.numpy as jnp
from jax import lax
from jax.experimental import pallas as pl
from jax.experimental.pallas import tpu as pltpu
from jax.sharding import Mesh, PartitionSpec as P

EPS = 1e-05
C0 = 0.7978845608028654
C1 = C0 * 0.044715
F32 = jnp.float32
BF16 = jnp.bfloat16
BLK = 128
PAIR = 256
CHUNK = 16
ROOT = BLK**0.5


def tanh_of(a):
    a2 = a * a
    return jnp.tanh(a * (C0 + C1 * a2)), a2


def gelu(a):
    t, _ = tanh_of(a)
    return a * (0.5 + 0.5 * t)


def gelu_and_slope(a):
    t, a2 = tanh_of(a)
    half = 0.5 + 0.5 * t
    value = a * half
    return value, half + value * (1.0 - half) * (2.0 * C0 + (6.0 * C1) * a2)


def norm(gated):
    centre = gated - jnp.mean(gated, axis=-1, keepdims=True)
    inverse = lax.rsqrt(jnp.sum(centre * centre, axis=-1, keepdims=True) + BLK * EPS)
    return centre * inverse, inverse


def lower_of(a):
    row = lax.broadcasted_iota(jnp.int32, a.shape, 0)
    col = lax.broadcasted_iota(jnp.int32, a.shape, 1)
    return jnp.where(row >= col, a, jnp.zeros_like(a))


def upright(row):
    return jnp.broadcast_to(row, (BLK, BLK)).T


def columns(ref, at, first=0, count=None):
    count = ref.shape[0] if count is None else count
    return jnp.concatenate([ref[first + k, at] for k in range(count)], axis=1)


def scatter_columns(src, dst, sem):
    @pl.loop(0, dst.shape[0])
    def _(k):
        at = pl.ds(pl.multiple_of(k * BLK, BLK), BLK)
        pltpu.make_async_copy(src.at[:, at], dst.at[k], sem).start()


def await_all(dst, sem):
    pltpu.make_async_copy(dst, dst, sem).wait()


def cols_of(g):
    return slice(g * BLK, (g + 1) * BLK)


def forward_kernel(
    order, u_ref, v_ref, d_hbm, w_ref, bias_ref, gain_ref, shift_ref, out_ref, d_ref, go_ref, low_at, bias_at, sem
):
    blocks, length, _ = d_ref.shape
    turns = length // PAIR
    step = pl.program_id(0)
    last = pl.num_programs(0) - 1
    now, before = lax.rem(step, 2), lax.rem(step + 1, 2)
    part = blocks // turns

    def multiply(i):
        out_ref[0, :, i * part * BLK : (i + 1) * part * BLK] = jnp.dot(
            go_ref[before],
            columns(d_ref, slice(None), i * part, part),
            preferred_element_type=F32,
        ).astype(out_ref.dtype)

    def gate(i):
        rows = [slice(i * PAIR + h * BLK, i * PAIR + (h + 1) * BLK) for h in range(2)]
        for g in range(2):
            gain, shift = ROOT * gain_ref[0, g : g + 1], shift_ref[0, g : g + 1]
            normed = []
            for at in rows:
                scaled, _ = norm(gelu(v_ref[at, cols_of(g)].astype(F32)))
                normed.append((scaled * gain + shift).astype(BF16))
            mixed = jnp.dot(
                low_at[g], jnp.concatenate(normed, axis=1), preferred_element_type=F32
            )
            for h, at in enumerate(rows):
                upper = gelu(u_ref[at, cols_of(g)].astype(F32))
                gated_out = (upper * (mixed[:, cols_of(h)] + bias_at[g])).astype(BF16)
                go_ref[now, cols_of(g), at] = gated_out.T

    @pl.when(step == 0)
    def _():
        scatter_columns(d_hbm, d_ref, sem)

    for g in range(2):
        bias_at[g] = upright(bias_ref[0, g : g + 1])
        low_at[g] = lower_of(w_ref[0, g].astype(F32)).astype(BF16)

    @pl.when(step == 0)
    def _():
        for i in range(turns):
            gate(i)
        await_all(d_ref, sem)

    @pl.when((step > 0) & (step < last))
    def _():
        for i in range(turns):
            multiply(i)
            gate(i)

    @pl.when(step == last)
    def _():
        for i in range(turns):
            multiply(i)


def forward(order, u, v, d, mix, bias, gain, shift):
    n = order.shape[0]
    length, width = u.shape
    last = n - 1
    cur = lambda j, o: (0, o[jnp.minimum(j, last)])
    par = lambda j, o: (o[jnp.minimum(j, last)], 0, 0)
    return pl.pallas_call(
        forward_kernel,
        grid_spec=pltpu.PrefetchScalarGridSpec(
            num_scalar_prefetch=1,
            grid=(n + 1,),
            in_specs=[
                pl.BlockSpec((length, PAIR), cur),
                pl.BlockSpec((length, PAIR), cur),
                pl.BlockSpec(memory_space=pl.ANY),
                pl.BlockSpec((1, 2, BLK, BLK), lambda j, o: (o[jnp.minimum(j, last)], 0, 0, 0)),
                pl.BlockSpec((1, 2, BLK), par),
                pl.BlockSpec((1, 2, BLK), par),
                pl.BlockSpec((1, 2, BLK), par),
            ],
            out_specs=pl.BlockSpec((1, PAIR, width), lambda j, o: (jnp.maximum(j - 1, 0), 0, 0)),
            scratch_shapes=[
                pltpu.VMEM((width // BLK, length, BLK), BF16),
                pltpu.VMEM((2, PAIR, length), BF16),
                pltpu.VMEM((2, BLK, BLK), BF16),
                pltpu.VMEM((2, BLK, BLK), F32),
                pltpu.SemaphoreType.DMA,
            ],
        ),
        out_shape=jax.ShapeDtypeStruct((n, PAIR, width), BF16),
        cost_estimate=pl.CostEstimate(
            flops=2 * n * PAIR * length * (width + BLK) * 2,
            bytes_accessed=length * width * 2 + n * PAIR * (4 * length + 2 * width),
            transcendentals=2 * n * PAIR * length,
        ),
        name="fwd",
    )(order, u, v, d, mix, bias, gain, shift)


def backward_kernel(
    pieces, order, u_ref, v_ref, d_hbm, mix_ref, bias_ref, gain_ref, shift_ref, *rest
):
    count = len(pieces)
    w_hbm = rest[:count]
    gu_ref, gv_ref, pack_ref = rest[-14:-11]
    d_ref, w_ref, cot_ref, low_at, turned_at, bias_at, b_acc, g_acc, s_acc, m_acc, sems = rest[-11:]
    turns = u_ref.shape[0] // PAIR
    step = pl.program_id(0)
    last = pl.num_programs(0) - 1

    def landing(k):
        slot, start, size = pieces[k]
        return w_ref.at[slot, :, pl.ds(start, size)]

    def cotangent(i, slot):
        return lax.dot_general(
            columns(d_ref, slice(i * PAIR, (i + 1) * PAIR)),
            columns(w_ref.at[slot], slice(None)),
            (((1,), (1,)), ((), ())),
            preferred_element_type=F32,
        )

    @pl.when(step == 0)
    def _():
        for k in range(count):
            if pieces[k][0] == 0:
                scatter_columns(w_hbm[k], landing(k), sems.at[k])
        scatter_columns(d_hbm, d_ref, sems.at[count])
        for k in range(count):
            if pieces[k][0] > 0:
                scatter_columns(w_hbm[k], landing(k), sems.at[k])
        for k in range(count):
            if pieces[k][0] == 0:
                await_all(landing(k), sems.at[k])
        await_all(d_ref, sems.at[count])
        cot_ref[0] = cotangent(0, 0)

    for k in range(count):
        if pieces[k][0] > 0:
            @pl.when(step == pieces[k][0] - 1)
            def _(k=k):
                await_all(landing(k), sems.at[k])

    for g in range(2):
        lower = lower_of(mix_ref[0, g].astype(F32))
        low_at[g] = lower.astype(BF16)
        turned_at[g] = lower.T.astype(BF16)
        bias_at[g] = upright(bias_ref[0, g : g + 1])
    b_acc[...] = jnp.zeros_like(b_acc)
    g_acc[...] = jnp.zeros_like(g_acc)
    s_acc[...] = jnp.zeros_like(s_acc)
    m_acc[...] = jnp.zeros_like(m_acc)
    for i in range(turns):
        if i + 1 < turns:
            cot_ref[(i + 1) % 2] = cotangent(i + 1, step)
        else:
            cot_ref[0] = cotangent(0, jnp.minimum(step + 1, last))
        for g in range(2):
            gain, shift = ROOT * gain_ref[0, g : g + 1], shift_ref[0, g : g + 1]
            rows = [slice(i * PAIR + h * BLK, i * PAIR + (h + 1) * BLK) for h in range(2)]
            kept, normed = [], []
            for at in rows:
                gated, slope = gelu_and_slope(v_ref[at, cols_of(g)].astype(F32))
                scaled, inverse = norm(gated)
                kept.append((scaled, inverse * slope))
                normed.append((scaled * gain + shift).astype(BF16))
            normed = jnp.concatenate(normed, axis=1)
            mixed = jnp.dot(low_at[g], normed, preferred_element_type=F32)
            d_mixed_b = []
            for h, at in enumerate(rows):
                upper, slope = gelu_and_slope(u_ref[at, cols_of(g)].astype(F32))
                cot = cot_ref[i % 2, h * BLK : (h + 1) * BLK, cols_of(g)]
                d_mixed = cot * upper
                d_mixed_b.append(d_mixed.astype(BF16))
                b_acc[g] += d_mixed
                gu_ref[at, cols_of(g)] = (
                    cot * slope * (mixed[:, cols_of(h)] + bias_at[g])
                ).astype(BF16)
            d_mixed_b = jnp.concatenate(d_mixed_b, axis=1)
            m_acc[g] += lax.dot_general(
                d_mixed_b, normed, (((1,), (1,)), ((), ())), preferred_element_type=F32
            )
            d_normed = jnp.dot(turned_at[g], d_mixed_b, preferred_element_type=F32)
            for h, at in enumerate(rows):
                scaled, scale = kept[h]
                dn = d_normed[:, cols_of(h)]
                weighted = dn * scaled
                g_acc[g] += jnp.sum(weighted.reshape(BLK // 8, 8, BLK), axis=0)
                s_acc[g] += jnp.sum(dn.reshape(BLK // 8, 8, BLK), axis=0)
                e = dn * gain
                mean_e = jnp.mean(e, axis=-1, keepdims=True)
                sum_es = jnp.sum(weighted * gain, axis=-1, keepdims=True)
                gv_ref[at, cols_of(g)] = (scale * (e - mean_e - scaled * sum_es)).astype(BF16)

    extra = []
    for g in range(2):
        extra.append(jnp.sum(b_acc[g].T, axis=0, keepdims=True))
        extra.append(ROOT * jnp.sum(g_acc[g], axis=0, keepdims=True))
        extra.append(jnp.sum(s_acc[g], axis=0, keepdims=True))
    row = lax.broadcasted_iota(jnp.int32, (BLK, BLK), 0)
    col = lax.broadcasted_iota(jnp.int32, (BLK, BLK), 1)
    extra.append(jnp.sum(jnp.where(row == col, m_acc[1], 0.0), axis=0, keepdims=True))
    both = jnp.where(row >= col, m_acc[0], m_acc[1].T)
    filler = jnp.zeros((CHUNK - 9, BLK), F32)
    blank = jnp.zeros((1, BLK), F32)
    for k in range(16):
        vector = extra[k] if k < len(extra) else blank
        pack_ref[0, k] = jnp.concatenate(
            [both[k * 8 : (k + 1) * 8], vector, filler], axis=0
        ).astype(BF16)


def unpack_kernel(x_ref, gw_ref, gb_ref, gg_ref, gs_ref):
    pair = pl.program_id(0)
    both = jnp.concatenate([x_ref[0, k, :8].astype(F32) for k in range(16)], axis=0)
    vector = lambda k: x_ref[0, k].astype(F32)[8:9]
    row = lax.broadcasted_iota(jnp.int32, (BLK, BLK), 0)
    col = lax.broadcasted_iota(jnp.int32, (BLK, BLK), 1)
    gw_ref[0] = jnp.where(row >= col, both, 0.0)
    turned = both.T
    gw_ref[1] = jnp.where(row > col, turned, jnp.where(row == col, vector(6), 0.0))
    for g in range(2):
        at = pl.ds(2 * pair + g, 1)
        gb_ref[at] = vector(3 * g)
        gg_ref[at] = vector(3 * g + 1)
        gs_ref[at] = vector(3 * g + 2)


def unpack(total):
    pairs = total.shape[0]
    whole = pl.BlockSpec((2 * pairs, BLK), lambda j: (0, 0))
    row = jax.ShapeDtypeStruct((2 * pairs, BLK), F32)
    return pl.pallas_call(
        unpack_kernel,
        grid=(pairs,),
        in_specs=[pl.BlockSpec((1, 16, CHUNK, BLK), lambda j: (j, 0, 0, 0))],
        out_specs=[pl.BlockSpec((2, BLK, BLK), lambda j: (j, 0, 0)), whole, whole, whole],
        out_shape=[jax.ShapeDtypeStruct((2 * pairs, BLK, BLK), F32), row, row, row],
        cost_estimate=pl.CostEstimate(flops=10**6, bytes_accessed=10**6, transcendentals=0),
        name="unpack",
    )(total)


def join_kernel(a_ref, b_ref, out_ref):
    out_ref[...] = (a_ref[...].astype(F32) + b_ref[...].astype(F32)).astype(BF16)


def join(a, b):
    n, rows, width = a.shape
    spec = pl.BlockSpec((1, rows // 2, width), lambda i, j: (i, j, 0))
    return pl.pallas_call(
        join_kernel,
        grid=(n, 2),
        in_specs=[spec, spec],
        out_specs=spec,
        out_shape=jax.ShapeDtypeStruct(a.shape, BF16),
        cost_estimate=pl.CostEstimate(
            flops=a.size, bytes_accessed=6 * a.size, transcendentals=0
        ),
        name="join",
    )(a, b)


def place_kernel(at, *refs):
    out_ref = refs[-1]
    for k, ref in enumerate(refs[:-1]):

        @pl.when(pl.program_id(0) == k)
        def _(ref=ref):
            n = ref.shape[0]
            for r in range(n):
                out_ref[0, lax.rem(at[1] - r + n, n)] = ref[r].astype(F32)


def place_rows(at, parts):
    n, (m, rows, width) = len(parts), parts[0].shape
    whole = pl.BlockSpec((m, rows, width), lambda k, at: (0, 0, 0))
    return pl.pallas_call(
        place_kernel,
        grid_spec=pltpu.PrefetchScalarGridSpec(
            num_scalar_prefetch=1,
            grid=(n,),
            in_specs=[whole] * n,
            out_specs=pl.BlockSpec(
                (1, m, rows, width), lambda k, at: (lax.rem(at[0] - k + n, n), 0, 0, 0)
            ),
        ),
        out_shape=jax.ShapeDtypeStruct((n, m, rows, width), F32),
        cost_estimate=pl.CostEstimate(
            flops=10**6, bytes_accessed=6 * n * m * rows * width, transcendentals=0
        ),
        name="place",
    )(at, *parts)


def backward(order, weights, u, v, d, mix, bias, gain, shift):
    n = order.shape[0]
    length, width = u.shape
    pairs = width // PAIR
    pieces = tuple((slot, start, w.shape[0]) for slot, start, w in weights)
    cur = lambda j, o: (0, o[j])
    par = lambda j, o: (o[j], 0, 0)
    mat = pl.BlockSpec((1, 2, BLK, BLK), lambda j, o: (o[j], 0, 0, 0))
    tile = pl.BlockSpec((length, PAIR), cur)
    vec = pl.BlockSpec((1, 2, BLK), par)
    hbm = pl.BlockSpec(memory_space=pl.ANY)
    shapes = [
        jax.ShapeDtypeStruct((length, width), BF16),
        jax.ShapeDtypeStruct((length, width), BF16),
        jax.ShapeDtypeStruct((pairs, 16, CHUNK, BLK), BF16),
    ]
    return pl.pallas_call(
        functools.partial(backward_kernel, pieces),
        grid_spec=pltpu.PrefetchScalarGridSpec(
            num_scalar_prefetch=1,
            grid=(n,),
            in_specs=[
                tile,
                tile,
                hbm,
                mat,
                vec,
                vec,
                vec,
                *[hbm] * len(weights),
            ],
            out_specs=[
                tile,
                tile,
                pl.BlockSpec((1, 16, CHUNK, BLK), lambda j, o: (o[j], 0, 0, 0)),
            ],
            scratch_shapes=[
                pltpu.VMEM((width // BLK, length, BLK), BF16),
                pltpu.VMEM((n, width // BLK, PAIR, BLK), BF16),
                pltpu.VMEM((2, PAIR, PAIR), F32),
                pltpu.VMEM((2, BLK, BLK), BF16),
                pltpu.VMEM((2, BLK, BLK), BF16),
                pltpu.VMEM((2, BLK, BLK), F32),
                pltpu.VMEM((2, BLK, BLK), F32),
                pltpu.VMEM((2, 8, BLK), F32),
                pltpu.VMEM((2, 8, BLK), F32),
                pltpu.VMEM((2, BLK, BLK), F32),
                pltpu.SemaphoreType.DMA((len(weights) + 1,)),
            ],
        ),
        out_shape=shapes,
        cost_estimate=pl.CostEstimate(
            flops=2 * n * PAIR * length * (width + 3 * BLK) * 2,
            bytes_accessed=length * width * 2 + n * PAIR * (8 * length + 2 * width),
            transcendentals=3 * n * PAIR * length,
        ),
        name="bwd",
    )(order, u, v, d, mix, bias, gain, shift, *[w for _, _, w in weights])


def hop(a, axis, size, by):
    return lax.ppermute(a, axis, [(i, (i + by) % size) for i in range(size)])


def added(a):
    return lax.optimization_barrier(jnp.sum(a.astype(F32), axis=0)).astype(BF16)


def spread(a, axes, count):
    return lax.all_to_all(jnp.broadcast_to(a[None], (count,) + a.shape), axes, 0, 0)


def on_device(u_pre, v_pre, d_out, w_mix, mix_bias, norm_gain, norm_shift, w_out, sizes=None):
    return everything(
        u_pre, v_pre, d_out, w_mix, mix_bias, norm_gain, norm_shift, w_out, sizes
    )


def everything(u_pre, v_pre, d_out, w_mix, mix_bias, norm_gain, norm_shift, w_out, sizes):
    nz, ny, nx, nc = sizes
    plane = nz * ny
    u, v, d = u_pre[0], v_pre[0], d_out[0]
    _, width = u.shape
    groups = w_mix.shape[0]
    pairs = groups // 2
    x, c = lax.axis_index("x"), lax.axis_index("c")
    xs = jnp.arange(nx, dtype=jnp.int32)

    swap = lambda a: hop(a, "c", nc, 1)
    half = w_out.shape[0] // 2
    own = swap(w_out)
    left = hop(w_out, "x", nx, 1)
    right = hop(w_out, "x", nx, -1)
    far0 = hop(left[:half], "x", nx, 1)
    far1 = hop(right[half:], "x", nx, -1)
    near = [swap(left), swap(right)]
    far = [swap(far0), swap(far1)]

    mix = w_mix.reshape(pairs, 2, BLK, BLK)
    bias = mix_bias.reshape(pairs, 2, BLK)
    gain = norm_gain.reshape(pairs, 2, BLK)
    shift = norm_shift.reshape(pairs, 2, BLK)

    common = (u, v, d, mix, bias, gain, shift)
    theirs = forward(xs * nc + (1 - c), *common)
    ours = forward(xs * nc + c, *common)
    traded = swap(theirs)
    joined = join(ours, traded)
    split = lax.all_to_all(joined.reshape(nx * plane, PAIR // plane, width), ("x", "z", "y"), 0, 0)

    place = lambda k, core: lax.rem(x + k, nx) * nc + core
    order = jnp.stack(
        [place(k, core) for ks in ((0,), (nx - 1, 1), (2,)) for core in (c, 1 - c) for k in ks]
    )
    weights = [
        (0, 0, w_out),
        (1, 0, own),
        (2, 0, left),
        (3, 0, right),
        (4, 0, near[0]),
        (5, 0, near[1]),
        (6, 0, far0),
        (6, half, far1),
        (7, 0, far[0]),
        (7, half, far[1]),
    ]
    grad_u, grad_v, packed = backward(order, weights, *common)

    packed, split = lax.optimization_barrier((packed, split))
    devices = nz * ny * nx * nc
    every = ("z", "y", "x", "c")
    packed = lax.all_to_all(packed.reshape(devices, CHUNK, BLK), every, 0, 0)
    rows = added(split)
    column = [rows] + [hop(rows, "y", ny, k) for k in range(1, ny)]
    column = jnp.stack(column)
    parts = [column] + [hop(column, "z", nz, k) for k in range(1, nz)]
    here = jnp.stack([lax.axis_index("z"), lax.axis_index("y")])
    grad_w_out = place_rows(here, parts).reshape(PAIR, width)
    total = spread(added(packed), every, devices)
    grad_w, *vectors = unpack(total.reshape(pairs, 16, CHUNK, BLK))
    return (grad_u[None], grad_v[None], grad_w_out, grad_w, *vectors)


def solution(mesh):
    devices = mesh.devices.reshape(4, -1, *[mesh.devices.shape[1] // 2, 2])
    grid = Mesh(devices, ("z", "y", "x", "c"))
    big = P(("x", "c"), ("z", "y"), None)
    rows = P(("x", "c"), None)
    return jax.shard_map(
        functools.partial(on_device, sizes=devices.shape),
        mesh=grid,
        in_specs=(big, big, big, P(), P(), P(), P(), rows),
        out_specs=(big, big, rows, P(), P(), P(), P()),
        check_vma=False,
    )
```

```python
import functools

import jax
import jax.numpy as jnp
from jax import lax
from jax.experimental import pallas as pl
from jax.experimental.pallas import tpu as pltpu
from jax.sharding import Mesh, PartitionSpec as P

EPS = 1e-05
C0 = 0.7978845608028654
C1 = C0 * 0.044715
F32 = jnp.float32
BF16 = jnp.bfloat16
BLK = 128
PAIR = 256
CHUNK = 16
ROOT = BLK**0.5


def tanh_of(a):
    a2 = a * a
    return jnp.tanh(a * (C0 + C1 * a2)), a2


def gelu(a):
    t, _ = tanh_of(a)
    return a * (0.5 + 0.5 * t)


def gelu_and_slope(a):
    t, a2 = tanh_of(a)
    half = 0.5 + 0.5 * t
    value = a * half
    return value, half + value * (1.0 - half) * (2.0 * C0 + (6.0 * C1) * a2)


def norm(gated):
    centre = gated - jnp.mean(gated, axis=-1, keepdims=True)
    inverse = lax.rsqrt(jnp.sum(centre * centre, axis=-1, keepdims=True) + BLK * EPS)
    return centre * inverse, inverse


def lower_of(a):
    row = lax.broadcasted_iota(jnp.int32, a.shape, 0)
    col = lax.broadcasted_iota(jnp.int32, a.shape, 1)
    return jnp.where(row >= col, a, jnp.zeros_like(a))


def upright(row):
    return jnp.broadcast_to(row, (BLK, BLK)).T


def columns(ref, at, first=0, count=None):
    count = ref.shape[0] if count is None else count
    return jnp.concatenate([ref[first + k, at] for k in range(count)], axis=1)


def scatter_columns(src, dst, sem):
    @pl.loop(0, dst.shape[0])
    def _(k):
        at = pl.ds(pl.multiple_of(k * BLK, BLK), BLK)
        pltpu.make_async_copy(src.at[:, at], dst.at[k], sem).start()


def await_all(dst, sem):
    pltpu.make_async_copy(dst, dst, sem).wait()


def cols_of(g):
    return slice(g * BLK, (g + 1) * BLK)


def forward_kernel(
    order, u_ref, v_ref, d_hbm, w_ref, bias_ref, gain_ref, shift_ref, out_ref, d_ref, go_ref, low_at, bias_at, sem
):
    blocks, length, _ = d_ref.shape
    turns = length // PAIR
    step = pl.program_id(0)
    last = pl.num_programs(0) - 1
    now, before = lax.rem(step, 2), lax.rem(step + 1, 2)
    part = blocks // turns

    def multiply(i):
        out_ref[0, :, i * part * BLK : (i + 1) * part * BLK] = jnp.dot(
            go_ref[before],
            columns(d_ref, slice(None), i * part, part),
            preferred_element_type=F32,
        ).astype(out_ref.dtype)

    def gate(i):
        rows = [slice(i * PAIR + h * BLK, i * PAIR + (h + 1) * BLK) for h in range(2)]
        for g in range(2):
            gain, shift = ROOT * gain_ref[0, g : g + 1], shift_ref[0, g : g + 1]
            normed = []
            for at in rows:
                scaled, _ = norm(gelu(v_ref[at, cols_of(g)].astype(F32)))
                normed.append((scaled * gain + shift).astype(BF16))
            mixed = jnp.dot(
                low_at[g], jnp.concatenate(normed, axis=1), preferred_element_type=F32
            )
            for h, at in enumerate(rows):
                upper = gelu(u_ref[at, cols_of(g)].astype(F32))
                gated_out = (upper * (mixed[:, cols_of(h)] + bias_at[g])).astype(BF16)
                go_ref[now, cols_of(g), at] = gated_out.T

    @pl.when(step == 0)
    def _():
        scatter_columns(d_hbm, d_ref, sem)

    for g in range(2):
        bias_at[g] = upright(bias_ref[0, g : g + 1])
        low_at[g] = lower_of(w_ref[0, g].astype(F32)).astype(BF16)

    @pl.when(step == 0)
    def _():
        for i in range(turns):
            gate(i)
        await_all(d_ref, sem)

    @pl.when((step > 0) & (step < last))
    def _():
        for i in range(turns):
            multiply(i)
            gate(i)

    @pl.when(step == last)
    def _():
        for i in range(turns):
            multiply(i)


def forward(order, u, v, d, mix, bias, gain, shift):
    n = order.shape[0]
    length, width = u.shape
    last = n - 1
    cur = lambda j, o: (0, o[jnp.minimum(j, last)])
    par = lambda j, o: (o[jnp.minimum(j, last)], 0, 0)
    return pl.pallas_call(
        forward_kernel,
        grid_spec=pltpu.PrefetchScalarGridSpec(
            num_scalar_prefetch=1,
            grid=(n + 1,),
            in_specs=[
                pl.BlockSpec((length, PAIR), cur),
                pl.BlockSpec((length, PAIR), cur),
                pl.BlockSpec(memory_space=pl.ANY),
                pl.BlockSpec((1, 2, BLK, BLK), lambda j, o: (o[jnp.minimum(j, last)], 0, 0, 0)),
                pl.BlockSpec((1, 2, BLK), par),
                pl.BlockSpec((1, 2, BLK), par),
                pl.BlockSpec((1, 2, BLK), par),
            ],
            out_specs=pl.BlockSpec((1, PAIR, width), lambda j, o: (jnp.maximum(j - 1, 0), 0, 0)),
            scratch_shapes=[
                pltpu.VMEM((width // BLK, length, BLK), BF16),
                pltpu.VMEM((2, PAIR, length), BF16),
                pltpu.VMEM((2, BLK, BLK), BF16),
                pltpu.VMEM((2, BLK, BLK), F32),
                pltpu.SemaphoreType.DMA,
            ],
        ),
        out_shape=jax.ShapeDtypeStruct((n, PAIR, width), BF16),
        cost_estimate=pl.CostEstimate(
            flops=2 * n * PAIR * length * (width + BLK) * 2,
            bytes_accessed=length * width * 2 + n * PAIR * (4 * length + 2 * width),
            transcendentals=2 * n * PAIR * length,
        ),
        name="fwd",
    )(order, u, v, d, mix, bias, gain, shift)


def backward_kernel(
    pieces, order, u_ref, v_ref, d_hbm, mix_ref, bias_ref, gain_ref, shift_ref, *rest
):
    count = len(pieces)
    w_hbm = rest[:count]
    gu_ref, gv_ref, pack_ref = rest[-14:-11]
    d_ref, w_ref, cot_ref, low_at, turned_at, bias_at, b_acc, g_acc, s_acc, m_acc, sems = rest[-11:]
    turns = u_ref.shape[0] // PAIR
    step = pl.program_id(0)
    last = pl.num_programs(0) - 1

    def landing(k):
        slot, start, size = pieces[k]
        return w_ref.at[slot, :, pl.ds(start, size)]

    def cotangent(i, slot):
        return lax.dot_general(
            columns(d_ref, slice(i * PAIR, (i + 1) * PAIR)),
            columns(w_ref.at[slot], slice(None)),
            (((1,), (1,)), ((), ())),
            preferred_element_type=F32,
        )

    @pl.when(step == 0)
    def _():
        for k in range(count):
            if pieces[k][0] == 0:
                scatter_columns(w_hbm[k], landing(k), sems.at[k])
        scatter_columns(d_hbm, d_ref, sems.at[count])
        for k in range(count):
            if pieces[k][0] > 0:
                scatter_columns(w_hbm[k], landing(k), sems.at[k])
        for k in range(count):
            if pieces[k][0] == 0:
                await_all(landing(k), sems.at[k])
        await_all(d_ref, sems.at[count])
        cot_ref[0] = cotangent(0, 0)

    for k in range(count):
        if pieces[k][0] > 0:
            @pl.when(step == pieces[k][0] - 1)
            def _(k=k):
                await_all(landing(k), sems.at[k])

    for g in range(2):
        lower = lower_of(mix_ref[0, g].astype(F32))
        low_at[g] = lower.astype(BF16)
        turned_at[g] = lower.T.astype(BF16)
        bias_at[g] = upright(bias_ref[0, g : g + 1])
    b_acc[...] = jnp.zeros_like(b_acc)
    g_acc[...] = jnp.zeros_like(g_acc)
    s_acc[...] = jnp.zeros_like(s_acc)
    m_acc[...] = jnp.zeros_like(m_acc)
    for i in range(turns):
        if i + 1 < turns:
            cot_ref[(i + 1) % 2] = cotangent(i + 1, step)
        else:
            cot_ref[0] = cotangent(0, jnp.minimum(step + 1, last))
        for g in range(2):
            gain, shift = ROOT * gain_ref[0, g : g + 1], shift_ref[0, g : g + 1]
            rows = [slice(i * PAIR + h * BLK, i * PAIR + (h + 1) * BLK) for h in range(2)]
            kept, normed = [], []
            for at in rows:
                gated, slope = gelu_and_slope(v_ref[at, cols_of(g)].astype(F32))
                scaled, inverse = norm(gated)
                kept.append((scaled, inverse * slope))
                normed.append((scaled * gain + shift).astype(BF16))
            normed = jnp.concatenate(normed, axis=1)
            mixed = jnp.dot(low_at[g], normed, preferred_element_type=F32)
            d_mixed_b = []
            for h, at in enumerate(rows):
                upper, slope = gelu_and_slope(u_ref[at, cols_of(g)].astype(F32))
                cot = cot_ref[i % 2, h * BLK : (h + 1) * BLK, cols_of(g)]
                d_mixed = cot * upper
                d_mixed_b.append(d_mixed.astype(BF16))
                b_acc[g] += d_mixed
                gu_ref[at, cols_of(g)] = (
                    cot * slope * (mixed[:, cols_of(h)] + bias_at[g])
                ).astype(BF16)
            d_mixed_b = jnp.concatenate(d_mixed_b, axis=1)
            m_acc[g] += lax.dot_general(
                d_mixed_b, normed, (((1,), (1,)), ((), ())), preferred_element_type=F32
            )
            d_normed = jnp.dot(turned_at[g], d_mixed_b, preferred_element_type=F32)
            for h, at in enumerate(rows):
                scaled, scale = kept[h]
                dn = d_normed[:, cols_of(h)]
                weighted = dn * scaled
                g_acc[g] += jnp.sum(weighted.reshape(BLK // 8, 8, BLK), axis=0)
                s_acc[g] += jnp.sum(dn.reshape(BLK // 8, 8, BLK), axis=0)
                e = dn * gain
                mean_e = jnp.mean(e, axis=-1, keepdims=True)
                sum_es = jnp.sum(weighted * gain, axis=-1, keepdims=True)
                gv_ref[at, cols_of(g)] = (scale * (e - mean_e - scaled * sum_es)).astype(BF16)

    extra = []
    for g in range(2):
        extra.append(jnp.sum(b_acc[g].T, axis=0, keepdims=True))
        extra.append(ROOT * jnp.sum(g_acc[g], axis=0, keepdims=True))
        extra.append(jnp.sum(s_acc[g], axis=0, keepdims=True))
    row = lax.broadcasted_iota(jnp.int32, (BLK, BLK), 0)
    col = lax.broadcasted_iota(jnp.int32, (BLK, BLK), 1)
    extra.append(jnp.sum(jnp.where(row == col, m_acc[1], 0.0), axis=0, keepdims=True))
    both = jnp.where(row >= col, m_acc[0], m_acc[1].T)
    filler = jnp.zeros((CHUNK - 9, BLK), F32)
    blank = jnp.zeros((1, BLK), F32)
    for k in range(16):
        vector = extra[k] if k < len(extra) else blank
        pack_ref[0, k] = jnp.concatenate(
            [both[k * 8 : (k + 1) * 8], vector, filler], axis=0
        ).astype(BF16)


def unpack_kernel(x_ref, gw_ref, gb_ref, gg_ref, gs_ref):
    chunks, pairs = x_ref.shape[:2]
    row = lax.broadcasted_iota(jnp.int32, (BLK, BLK), 0)
    col = lax.broadcasted_iota(jnp.int32, (BLK, BLK), 1)

    @pl.loop(0, pairs)
    def _(pair):
        part = [x_ref[k, pair].astype(F32) for k in range(chunks)]
        both = jnp.concatenate([p[:8] for p in part], axis=0)
        vector = lambda k: part[k][8:9]
        gw_ref[2 * pair] = jnp.where(row >= col, both, 0.0)
        gw_ref[2 * pair + 1] = jnp.where(
            row > col, both.T, jnp.where(row == col, vector(6), 0.0)
        )
        for g in range(2):
            at = pl.ds(2 * pair + g, 1)
            gb_ref[at] = vector(3 * g)
            gg_ref[at] = vector(3 * g + 1)
            gs_ref[at] = vector(3 * g + 2)


def unpack(total):
    pairs = total.shape[1]
    row = jax.ShapeDtypeStruct((2 * pairs, BLK), F32)
    return pl.pallas_call(
        unpack_kernel,
        out_shape=[jax.ShapeDtypeStruct((2 * pairs, BLK, BLK), F32), row, row, row],
        cost_estimate=pl.CostEstimate(flops=10**6, bytes_accessed=10**6, transcendentals=0),
        name="unpack",
    )(total)


def join_kernel(a_hbm, b_hbm, out_hbm, a_ref, b_ref, out_ref, sems):
    count = a_hbm.shape[0]
    hbm = (a_hbm, b_hbm, out_hbm)
    vmem = (a_ref, b_ref, out_ref)
    read = lambda s, k: pltpu.make_async_copy(hbm[s].at[k], vmem[s].at[k], sems.at[s, k])
    write = lambda k: pltpu.make_async_copy(out_ref.at[k], out_hbm.at[k], sems.at[2, k])

    for k in range(count):
        read(0, k).start()
        read(1, k).start()

    @pl.loop(0, count)
    def _(k):
        read(0, k).wait()
        read(1, k).wait()
        out_ref[k] = (a_ref[k].astype(F32) + b_ref[k].astype(F32)).astype(BF16)
        write(k).start()

    for k in range(count):
        write(k).wait()


def join(a, b):
    n, rows, width = a.shape
    parts = (4 * n, rows // 4, width)
    hbm = pl.BlockSpec(memory_space=pl.ANY)
    return pl.pallas_call(
        join_kernel,
        in_specs=[hbm, hbm],
        out_specs=hbm,
        out_shape=jax.ShapeDtypeStruct(parts, BF16),
        scratch_shapes=[pltpu.VMEM(parts, BF16)] * 3 + [pltpu.SemaphoreType.DMA((3, 4 * n))],
        cost_estimate=pl.CostEstimate(
            flops=a.size, bytes_accessed=6 * a.size, transcendentals=0
        ),
        name="join",
    )(a.reshape(parts), b.reshape(parts)).reshape(a.shape)


def place_kernel(at, *refs):
    out_ref = refs[-1]
    for k, ref in enumerate(refs[:-1]):

        @pl.when(pl.program_id(0) == k)
        def _(ref=ref):
            n = ref.shape[0]
            for r in range(n):
                out_ref[0, lax.rem(at[1] - r + n, n)] = ref[r].astype(F32)


def place_rows(at, parts):
    n, (m, rows, width) = len(parts), parts[0].shape
    whole = pl.BlockSpec((m, rows, width), lambda k, at: (0, 0, 0))
    return pl.pallas_call(
        place_kernel,
        grid_spec=pltpu.PrefetchScalarGridSpec(
            num_scalar_prefetch=1,
            grid=(n,),
            in_specs=[whole] * n,
            out_specs=pl.BlockSpec(
                (1, m, rows, width), lambda k, at: (lax.rem(at[0] - k + n, n), 0, 0, 0)
            ),
        ),
        out_shape=jax.ShapeDtypeStruct((n, m, rows, width), F32),
        cost_estimate=pl.CostEstimate(
            flops=10**6, bytes_accessed=6 * n * m * rows * width, transcendentals=0
        ),
        name="place",
    )(at, *parts)


def backward(order, weights, u, v, d, mix, bias, gain, shift):
    n = order.shape[0]
    length, width = u.shape
    pairs = width // PAIR
    pieces = tuple((slot, start, w.shape[0]) for slot, start, w in weights)
    cur = lambda j, o: (0, o[j])
    par = lambda j, o: (o[j], 0, 0)
    mat = pl.BlockSpec((1, 2, BLK, BLK), lambda j, o: (o[j], 0, 0, 0))
    tile = pl.BlockSpec((length, PAIR), cur)
    vec = pl.BlockSpec((1, 2, BLK), par)
    hbm = pl.BlockSpec(memory_space=pl.ANY)
    shapes = [
        jax.ShapeDtypeStruct((length, width), BF16),
        jax.ShapeDtypeStruct((length, width), BF16),
        jax.ShapeDtypeStruct((pairs, 16, CHUNK, BLK), BF16),
    ]
    return pl.pallas_call(
        functools.partial(backward_kernel, pieces),
        grid_spec=pltpu.PrefetchScalarGridSpec(
            num_scalar_prefetch=1,
            grid=(n,),
            in_specs=[
                tile,
                tile,
                hbm,
                mat,
                vec,
                vec,
                vec,
                *[hbm] * len(weights),
            ],
            out_specs=[
                tile,
                tile,
                pl.BlockSpec((1, 16, CHUNK, BLK), lambda j, o: (j, 0, 0, 0)),
            ],
            scratch_shapes=[
                pltpu.VMEM((width // BLK, length, BLK), BF16),
                pltpu.VMEM((n, width // BLK, PAIR, BLK), BF16),
                pltpu.VMEM((2, PAIR, PAIR), F32),
                pltpu.VMEM((2, BLK, BLK), BF16),
                pltpu.VMEM((2, BLK, BLK), BF16),
                pltpu.VMEM((2, BLK, BLK), F32),
                pltpu.VMEM((2, BLK, BLK), F32),
                pltpu.VMEM((2, 8, BLK), F32),
                pltpu.VMEM((2, 8, BLK), F32),
                pltpu.VMEM((2, BLK, BLK), F32),
                pltpu.SemaphoreType.DMA((len(weights) + 1,)),
            ],
        ),
        out_shape=shapes,
        cost_estimate=pl.CostEstimate(
            flops=2 * n * PAIR * length * (width + 3 * BLK) * 2,
            bytes_accessed=length * width * 2 + n * PAIR * (8 * length + 2 * width),
            transcendentals=3 * n * PAIR * length,
        ),
        name="bwd",
    )(order, u, v, d, mix, bias, gain, shift, *[w for _, _, w in weights])


def hop(a, axis, size, by):
    return lax.ppermute(a, axis, [(i, (i + by) % size) for i in range(size)])


def added(a):
    return lax.optimization_barrier(jnp.sum(a.astype(F32), axis=0)).astype(BF16)


def spread(a, axes, count):
    return lax.all_to_all(jnp.broadcast_to(a[None], (count,) + a.shape), axes, 0, 0)


def on_device(u_pre, v_pre, d_out, w_mix, mix_bias, norm_gain, norm_shift, w_out, sizes=None):
    return everything(
        u_pre, v_pre, d_out, w_mix, mix_bias, norm_gain, norm_shift, w_out, sizes
    )


def everything(u_pre, v_pre, d_out, w_mix, mix_bias, norm_gain, norm_shift, w_out, sizes):
    nz, ny, nx, nc = sizes
    plane = nz * ny
    u, v, d = u_pre[0], v_pre[0], d_out[0]
    _, width = u.shape
    groups = w_mix.shape[0]
    pairs = groups // 2
    x, c = lax.axis_index("x"), lax.axis_index("c")
    xs = jnp.arange(nx, dtype=jnp.int32)

    swap = lambda a: hop(a, "c", nc, 1)
    half = w_out.shape[0] // 2
    own = swap(w_out)
    left = hop(w_out, "x", nx, 1)
    right = hop(w_out, "x", nx, -1)
    far0 = hop(left[:half], "x", nx, 1)
    far1 = hop(right[half:], "x", nx, -1)
    near = [swap(left), swap(right)]
    far = [swap(far0), swap(far1)]

    mix = w_mix.reshape(pairs, 2, BLK, BLK)
    bias = mix_bias.reshape(pairs, 2, BLK)
    gain = norm_gain.reshape(pairs, 2, BLK)
    shift = norm_shift.reshape(pairs, 2, BLK)

    common = (u, v, d, mix, bias, gain, shift)
    theirs = forward(xs * nc + (1 - c), *common)
    ours = forward(xs * nc + c, *common)
    traded = swap(theirs)
    joined = join(ours, traded)
    split = lax.all_to_all(joined.reshape(nx * plane, PAIR // plane, width), ("x", "z", "y"), 0, 0)

    place = lambda k, core: lax.rem(x + k, nx) * nc + core
    hops = (0, nx - 1, 1, 2)
    order = jnp.stack([place(k, core) for core in (1 - c, c) for k in hops])
    weights = [
        (0, 0, own),
        (1, 0, near[0]),
        (2, 0, near[1]),
        (3, 0, far[0]),
        (3, half, far[1]),
        (4, 0, w_out),
        (5, 0, left),
        (6, 0, right),
        (7, 0, far0),
        (7, half, far1),
    ]
    grad_u, grad_v, packed = backward(order, weights, *common)

    mine = packed[nx:].astype(F32) + swap(packed[:nx]).astype(F32)
    mine = lax.optimization_barrier(mine).astype(BF16)
    arrived = [hop(mine[1], "x", nx, -1), hop(mine[2], "x", nx, 1), hop(mine[3], "x", nx, 2)]
    ours = mine[0].astype(F32)
    for a in arrived:
        ours = ours + a.astype(F32)
    ours = lax.optimization_barrier(ours).astype(BF16)

    ours, split = lax.optimization_barrier((ours, split))
    devices = nz * ny * nx * nc
    rows = added(split)
    column = [rows] + [hop(rows, "y", ny, k) for k in range(1, ny)]
    column = jnp.stack(column)
    parts = [column] + [hop(column, "z", nz, k) for k in range(1, nz)]
    here = jnp.stack([lax.axis_index("z"), lax.axis_index("y")])
    grad_w_out = place_rows(here, parts).reshape(PAIR, width)
    ours = lax.all_to_all(ours, ("z", "y"), 0, 0)
    total = spread(added(ours), ("z", "y", "x", "c"), devices)
    grad_w, *vectors = unpack(total.reshape(plane, pairs, CHUNK, BLK))
    return (grad_u[None], grad_v[None], grad_w_out, grad_w, *vectors)


def solution(mesh):
    devices = mesh.devices.reshape(4, -1, *[mesh.devices.shape[1] // 2, 2])
    grid = Mesh(devices, ("z", "y", "x", "c"))
    big = P(("x", "c"), ("z", "y"), None)
    rows = P(("x", "c"), None)
    return jax.shard_map(
        functools.partial(on_device, sizes=devices.shape),
        mesh=grid,
        in_specs=(big, big, big, P(), P(), P(), P(), rows),
        out_specs=(big, big, rows, P(), P(), P(), P()),
        check_vma=False,
    )
```

```python
import functools

import jax
import jax.numpy as jnp
from jax import lax
from jax.experimental import pallas as pl
from jax.experimental.pallas import tpu as pltpu
from jax.sharding import Mesh, PartitionSpec as P

EPS = 1e-05
C0 = 0.7978845608028654
C1 = C0 * 0.044715
F32 = jnp.float32
BF16 = jnp.bfloat16
BLK = 128
PAIR = 256
CHUNK = 16
ROOT = BLK**0.5


def tanh_of(a):
    a2 = a * a
    return jnp.tanh(a * (C0 + C1 * a2)), a2


def gelu(a):
    t, _ = tanh_of(a)
    return a * (0.5 + 0.5 * t)


def gelu_and_slope(a):
    t, a2 = tanh_of(a)
    half = 0.5 + 0.5 * t
    value = a * half
    return value, half + value * (1.0 - half) * (2.0 * C0 + (6.0 * C1) * a2)


def norm(gated):
    centre = gated - jnp.mean(gated, axis=-1, keepdims=True)
    inverse = lax.rsqrt(jnp.sum(centre * centre, axis=-1, keepdims=True) + BLK * EPS)
    return centre * inverse, inverse


def lower_of(a):
    row = lax.broadcasted_iota(jnp.int32, a.shape, 0)
    col = lax.broadcasted_iota(jnp.int32, a.shape, 1)
    return jnp.where(row >= col, a, jnp.zeros_like(a))


def upright(row):
    return jnp.broadcast_to(row, (BLK, BLK)).T


def columns(ref, at, first=0, count=None):
    count = ref.shape[0] if count is None else count
    return jnp.concatenate([ref[first + k, at] for k in range(count)], axis=1)


def scatter_columns(src, dst, sem):
    @pl.loop(0, dst.shape[0])
    def _(k):
        at = pl.ds(pl.multiple_of(k * BLK, BLK), BLK)
        pltpu.make_async_copy(src.at[:, at], dst.at[k], sem).start()


def await_all(dst, sem):
    pltpu.make_async_copy(dst, dst, sem).wait()


def cols_of(g):
    return slice(g * BLK, (g + 1) * BLK)


def forward_kernel(
    order, u_ref, v_ref, d_hbm, w_ref, bias_ref, gain_ref, shift_ref, out_ref, d_ref, go_ref, low_at, bias_at, sem
):
    blocks, length, _ = d_ref.shape
    turns = length // PAIR
    step = pl.program_id(0)
    last = pl.num_programs(0) - 1
    now, before = lax.rem(step, 2), lax.rem(step + 1, 2)
    part = blocks // turns

    def multiply(i):
        out_ref[0, :, i * part * BLK : (i + 1) * part * BLK] = jnp.dot(
            go_ref[before],
            columns(d_ref, slice(None), i * part, part),
            preferred_element_type=F32,
        ).astype(out_ref.dtype)

    def gate(i):
        rows = [slice(i * PAIR + h * BLK, i * PAIR + (h + 1) * BLK) for h in range(2)]
        for g in range(2):
            gain, shift = ROOT * gain_ref[0, g : g + 1], shift_ref[0, g : g + 1]
            normed = []
            for at in rows:
                scaled, _ = norm(gelu(v_ref[at, cols_of(g)].astype(F32)))
                normed.append((scaled * gain + shift).astype(BF16))
            mixed = jnp.dot(
                low_at[g], jnp.concatenate(normed, axis=1), preferred_element_type=F32
            )
            for h, at in enumerate(rows):
                upper = gelu(u_ref[at, cols_of(g)].astype(F32))
                gated_out = (upper * (mixed[:, cols_of(h)] + bias_at[g])).astype(BF16)
                go_ref[now, cols_of(g), at] = gated_out.T

    @pl.when(step == 0)
    def _():
        scatter_columns(d_hbm, d_ref, sem)

    for g in range(2):
        bias_at[g] = upright(bias_ref[0, g : g + 1])
        low_at[g] = lower_of(w_ref[0, g].astype(F32)).astype(BF16)

    @pl.when(step == 0)
    def _():
        for i in range(turns):
            gate(i)
        await_all(d_ref, sem)

    @pl.when((step > 0) & (step < last))
    def _():
        for i in range(turns):
            multiply(i)
            gate(i)

    @pl.when(step == last)
    def _():
        for i in range(turns):
            multiply(i)


def forward(order, u, v, d, mix, bias, gain, shift):
    n = order.shape[0]
    length, width = u.shape
    last = n - 1
    cur = lambda j, o: (0, o[jnp.minimum(j, last)])
    par = lambda j, o: (o[jnp.minimum(j, last)], 0, 0)
    return pl.pallas_call(
        forward_kernel,
        grid_spec=pltpu.PrefetchScalarGridSpec(
            num_scalar_prefetch=1,
            grid=(n + 1,),
            in_specs=[
                pl.BlockSpec((length, PAIR), cur),
                pl.BlockSpec((length, PAIR), cur),
                pl.BlockSpec(memory_space=pl.ANY),
                pl.BlockSpec((1, 2, BLK, BLK), lambda j, o: (o[jnp.minimum(j, last)], 0, 0, 0)),
                pl.BlockSpec((1, 2, BLK), par),
                pl.BlockSpec((1, 2, BLK), par),
                pl.BlockSpec((1, 2, BLK), par),
            ],
            out_specs=pl.BlockSpec((1, PAIR, width), lambda j, o: (jnp.maximum(j - 1, 0), 0, 0)),
            scratch_shapes=[
                pltpu.VMEM((width // BLK, length, BLK), BF16),
                pltpu.VMEM((2, PAIR, length), BF16),
                pltpu.VMEM((2, BLK, BLK), BF16),
                pltpu.VMEM((2, BLK, BLK), F32),
                pltpu.SemaphoreType.DMA,
            ],
        ),
        out_shape=jax.ShapeDtypeStruct((n, PAIR, width), BF16),
        cost_estimate=pl.CostEstimate(
            flops=2 * n * PAIR * length * (width + BLK) * 2,
            bytes_accessed=length * width * 2 + n * PAIR * (4 * length + 2 * width),
            transcendentals=2 * n * PAIR * length,
        ),
        name="fwd",
    )(order, u, v, d, mix, bias, gain, shift)


def backward_kernel(
    pieces, order, u_ref, v_ref, d_hbm, mix_ref, bias_ref, gain_ref, shift_ref, *rest
):
    count = len(pieces)
    w_hbm = rest[:count]
    gu_ref, gv_ref, pack_ref = rest[-14:-11]
    d_ref, w_ref, cot_ref, low_at, turned_at, bias_at, b_acc, g_acc, s_acc, m_acc, sems = rest[-11:]
    turns = u_ref.shape[0] // PAIR
    step = pl.program_id(0)
    last = pl.num_programs(0) - 1

    def landing(k):
        slot, start, size = pieces[k]
        return w_ref.at[slot, :, pl.ds(start, size)]

    def cotangent(i, slot):
        return lax.dot_general(
            columns(d_ref, slice(i * PAIR, (i + 1) * PAIR)),
            columns(w_ref.at[slot], slice(None)),
            (((1,), (1,)), ((), ())),
            preferred_element_type=F32,
        )

    @pl.when(step == 0)
    def _():
        for k in range(count):
            if pieces[k][0] == 0:
                scatter_columns(w_hbm[k], landing(k), sems.at[k])
        scatter_columns(d_hbm, d_ref, sems.at[count])
        for k in range(count):
            if pieces[k][0] > 0:
                scatter_columns(w_hbm[k], landing(k), sems.at[k])
        for k in range(count):
            if pieces[k][0] == 0:
                await_all(landing(k), sems.at[k])
        await_all(d_ref, sems.at[count])
        cot_ref[0] = cotangent(0, 0)

    for k in range(count):
        if pieces[k][0] > 0:
            @pl.when(step == pieces[k][0] - 1)
            def _(k=k):
                await_all(landing(k), sems.at[k])

    for g in range(2):
        lower = lower_of(mix_ref[0, g].astype(F32))
        low_at[g] = lower.astype(BF16)
        turned_at[g] = lower.T.astype(BF16)
        bias_at[g] = upright(bias_ref[0, g : g + 1])
    b_acc[...] = jnp.zeros_like(b_acc)
    g_acc[...] = jnp.zeros_like(g_acc)
    s_acc[...] = jnp.zeros_like(s_acc)
    m_acc[...] = jnp.zeros_like(m_acc)
    for i in range(turns):
        if i + 1 < turns:
            cot_ref[(i + 1) % 2] = cotangent(i + 1, step)
        else:
            cot_ref[0] = cotangent(0, jnp.minimum(step + 1, last))
        for g in range(2):
            gain, shift = ROOT * gain_ref[0, g : g + 1], shift_ref[0, g : g + 1]
            rows = [slice(i * PAIR + h * BLK, i * PAIR + (h + 1) * BLK) for h in range(2)]
            kept, normed = [], []
            for at in rows:
                gated, slope = gelu_and_slope(v_ref[at, cols_of(g)].astype(F32))
                scaled, inverse = norm(gated)
                kept.append((scaled, inverse * slope))
                normed.append((scaled * gain + shift).astype(BF16))
            normed = jnp.concatenate(normed, axis=1)
            mixed = jnp.dot(low_at[g], normed, preferred_element_type=F32)
            d_mixed_b = []
            for h, at in enumerate(rows):
                upper, slope = gelu_and_slope(u_ref[at, cols_of(g)].astype(F32))
                cot = cot_ref[i % 2, h * BLK : (h + 1) * BLK, cols_of(g)]
                d_mixed = cot * upper
                d_mixed_b.append(d_mixed.astype(BF16))
                b_acc[g] += d_mixed
                gu_ref[at, cols_of(g)] = (
                    cot * slope * (mixed[:, cols_of(h)] + bias_at[g])
                ).astype(BF16)
            d_mixed_b = jnp.concatenate(d_mixed_b, axis=1)
            m_acc[g] += lax.dot_general(
                d_mixed_b, normed, (((1,), (1,)), ((), ())), preferred_element_type=F32
            )
            d_normed = jnp.dot(turned_at[g], d_mixed_b, preferred_element_type=F32)
            for h, at in enumerate(rows):
                scaled, scale = kept[h]
                dn = d_normed[:, cols_of(h)]
                weighted = dn * scaled
                g_acc[g] += jnp.sum(weighted.reshape(BLK // 8, 8, BLK), axis=0)
                s_acc[g] += jnp.sum(dn.reshape(BLK // 8, 8, BLK), axis=0)
                e = dn * gain
                mean_e = jnp.mean(e, axis=-1, keepdims=True)
                sum_es = jnp.sum(weighted * gain, axis=-1, keepdims=True)
                gv_ref[at, cols_of(g)] = (scale * (e - mean_e - scaled * sum_es)).astype(BF16)

    extra = []
    for g in range(2):
        extra.append(jnp.sum(b_acc[g].T, axis=0, keepdims=True))
        extra.append(ROOT * jnp.sum(g_acc[g], axis=0, keepdims=True))
        extra.append(jnp.sum(s_acc[g], axis=0, keepdims=True))
    row = lax.broadcasted_iota(jnp.int32, (BLK, BLK), 0)
    col = lax.broadcasted_iota(jnp.int32, (BLK, BLK), 1)
    extra.append(jnp.sum(jnp.where(row == col, m_acc[1], 0.0), axis=0, keepdims=True))
    both = jnp.where(row >= col, m_acc[0], m_acc[1].T)
    filler = jnp.zeros((CHUNK - 9, BLK), F32)
    blank = jnp.zeros((1, BLK), F32)
    for k in range(16):
        vector = extra[k] if k < len(extra) else blank
        pack_ref[0, k] = jnp.concatenate(
            [both[k * 8 : (k + 1) * 8], vector, filler], axis=0
        ).astype(BF16)


def unpack_kernel(x_ref, gw_ref, gb_ref, gg_ref, gs_ref):
    chunks, pairs = x_ref.shape[:2]
    row = lax.broadcasted_iota(jnp.int32, (BLK, BLK), 0)
    col = lax.broadcasted_iota(jnp.int32, (BLK, BLK), 1)

    @pl.loop(0, pairs)
    def _(pair):
        part = [x_ref[k, pair].astype(F32) for k in range(chunks)]
        both = jnp.concatenate([p[:8] for p in part], axis=0)
        vector = lambda k: part[k][8:9]
        gw_ref[2 * pair] = jnp.where(row >= col, both, 0.0)
        gw_ref[2 * pair + 1] = jnp.where(
            row > col, both.T, jnp.where(row == col, vector(6), 0.0)
        )
        for g in range(2):
            at = pl.ds(2 * pair + g, 1)
            gb_ref[at] = vector(3 * g)
            gg_ref[at] = vector(3 * g + 1)
            gs_ref[at] = vector(3 * g + 2)


def unpack(total):
    pairs = total.shape[1]
    row = jax.ShapeDtypeStruct((2 * pairs, BLK), F32)
    return pl.pallas_call(
        unpack_kernel,
        out_shape=[jax.ShapeDtypeStruct((2 * pairs, BLK, BLK), F32), row, row, row],
        cost_estimate=pl.CostEstimate(flops=10**6, bytes_accessed=10**6, transcendentals=0),
        name="unpack",
    )(total)


def join_kernel(a_hbm, b_hbm, out_hbm, a_ref, b_ref, out_ref, sems):
    count = a_hbm.shape[0]
    hbm = (a_hbm, b_hbm, out_hbm)
    vmem = (a_ref, b_ref, out_ref)
    read = lambda s, k: pltpu.make_async_copy(hbm[s].at[k], vmem[s].at[k], sems.at[s, k])
    write = lambda k: pltpu.make_async_copy(out_ref.at[k], out_hbm.at[k], sems.at[2, k])

    for k in range(count):
        read(0, k).start()
        read(1, k).start()

    @pl.loop(0, count)
    def _(k):
        read(0, k).wait()
        read(1, k).wait()
        out_ref[k] = (a_ref[k].astype(F32) + b_ref[k].astype(F32)).astype(BF16)
        write(k).start()

    for k in range(count):
        write(k).wait()


def join(a, b):
    n, rows, width = a.shape
    parts = (4 * n, rows // 4, width)
    hbm = pl.BlockSpec(memory_space=pl.ANY)
    return pl.pallas_call(
        join_kernel,
        in_specs=[hbm, hbm],
        out_specs=hbm,
        out_shape=jax.ShapeDtypeStruct(parts, BF16),
        scratch_shapes=[pltpu.VMEM(parts, BF16)] * 3 + [pltpu.SemaphoreType.DMA((3, 4 * n))],
        cost_estimate=pl.CostEstimate(
            flops=a.size, bytes_accessed=6 * a.size, transcendentals=0
        ),
        name="join",
    )(a.reshape(parts), b.reshape(parts)).reshape(a.shape)


def backward(order, weights, u, v, d, mix, bias, gain, shift):
    n = order.shape[0]
    length, width = u.shape
    pairs = width // PAIR
    pieces = tuple((slot, start, w.shape[0]) for slot, start, w in weights)
    cur = lambda j, o: (0, o[j])
    par = lambda j, o: (o[j], 0, 0)
    mat = pl.BlockSpec((1, 2, BLK, BLK), lambda j, o: (o[j], 0, 0, 0))
    tile = pl.BlockSpec((length, PAIR), cur)
    vec = pl.BlockSpec((1, 2, BLK), par)
    hbm = pl.BlockSpec(memory_space=pl.ANY)
    shapes = [
        jax.ShapeDtypeStruct((length, width), BF16),
        jax.ShapeDtypeStruct((length, width), BF16),
        jax.ShapeDtypeStruct((pairs, 16, CHUNK, BLK), BF16),
    ]
    return pl.pallas_call(
        functools.partial(backward_kernel, pieces),
        grid_spec=pltpu.PrefetchScalarGridSpec(
            num_scalar_prefetch=1,
            grid=(n,),
            in_specs=[
                tile,
                tile,
                hbm,
                mat,
                vec,
                vec,
                vec,
                *[hbm] * len(weights),
            ],
            out_specs=[
                tile,
                tile,
                pl.BlockSpec((1, 16, CHUNK, BLK), lambda j, o: (j, 0, 0, 0)),
            ],
            scratch_shapes=[
                pltpu.VMEM((width // BLK, length, BLK), BF16),
                pltpu.VMEM((n, width // BLK, PAIR, BLK), BF16),
                pltpu.VMEM((2, PAIR, PAIR), F32),
                pltpu.VMEM((2, BLK, BLK), BF16),
                pltpu.VMEM((2, BLK, BLK), BF16),
                pltpu.VMEM((2, BLK, BLK), F32),
                pltpu.VMEM((2, BLK, BLK), F32),
                pltpu.VMEM((2, 8, BLK), F32),
                pltpu.VMEM((2, 8, BLK), F32),
                pltpu.VMEM((2, BLK, BLK), F32),
                pltpu.SemaphoreType.DMA((len(weights) + 1,)),
            ],
        ),
        out_shape=shapes,
        cost_estimate=pl.CostEstimate(
            flops=2 * n * PAIR * length * (width + 3 * BLK) * 2,
            bytes_accessed=length * width * 2 + n * PAIR * (8 * length + 2 * width),
            transcendentals=3 * n * PAIR * length,
        ),
        name="bwd",
    )(order, u, v, d, mix, bias, gain, shift, *[w for _, _, w in weights])


def hop(a, axis, size, by):
    return lax.ppermute(a, axis, [(i, (i + by) % size) for i in range(size)])


def added(a):
    return lax.optimization_barrier(jnp.sum(a.astype(F32), axis=0)).astype(BF16)


def spread(a, axes, count):
    return lax.all_to_all(jnp.broadcast_to(a[None], (count,) + a.shape), axes, 0, 0)


def on_device(u_pre, v_pre, d_out, w_mix, mix_bias, norm_gain, norm_shift, w_out, sizes=None):
    return everything(
        u_pre, v_pre, d_out, w_mix, mix_bias, norm_gain, norm_shift, w_out, sizes
    )


def everything(u_pre, v_pre, d_out, w_mix, mix_bias, norm_gain, norm_shift, w_out, sizes):
    nz, ny, nx, nc = sizes
    plane = nz * ny
    u, v, d = u_pre[0], v_pre[0], d_out[0]
    _, width = u.shape
    groups = w_mix.shape[0]
    pairs = groups // 2
    x, c = lax.axis_index("x"), lax.axis_index("c")
    xs = jnp.arange(nx, dtype=jnp.int32)

    swap = lambda a: hop(a, "c", nc, 1)
    half = w_out.shape[0] // 2
    own = swap(w_out)
    left = hop(w_out, "x", nx, 1)
    right = hop(w_out, "x", nx, -1)
    far0 = hop(left[:half], "x", nx, 1)
    far1 = hop(right[half:], "x", nx, -1)
    near = [swap(left), swap(right)]
    far = [swap(far0), swap(far1)]

    mix = w_mix.reshape(pairs, 2, BLK, BLK)
    bias = mix_bias.reshape(pairs, 2, BLK)
    gain = norm_gain.reshape(pairs, 2, BLK)
    shift = norm_shift.reshape(pairs, 2, BLK)

    common = (u, v, d, mix, bias, gain, shift)
    theirs = forward(xs * nc + (1 - c), *common)
    ours = forward(xs * nc + c, *common)
    traded = swap(theirs)
    joined = join(ours, traded)
    split = lax.all_to_all(joined.reshape(nx * plane, PAIR // plane, width), ("x", "z", "y"), 0, 0)

    place = lambda k, core: lax.rem(x + k, nx) * nc + core
    hops = (0, nx - 1, 1, 2)
    order = jnp.stack([place(k, core) for core in (1 - c, c) for k in hops])
    weights = [
        (0, 0, own),
        (1, 0, near[0]),
        (2, 0, near[1]),
        (3, 0, far[0]),
        (3, half, far[1]),
        (4, 0, w_out),
        (5, 0, left),
        (6, 0, right),
        (7, 0, far0),
        (7, half, far1),
    ]
    grad_u, grad_v, packed = backward(order, weights, *common)

    mine = packed[nx:].astype(F32) + swap(packed[:nx]).astype(F32)
    mine = lax.optimization_barrier(mine).astype(BF16)
    arrived = [hop(mine[1], "x", nx, -1), hop(mine[2], "x", nx, 1), hop(mine[3], "x", nx, 2)]
    ours = mine[0].astype(F32)
    for a in arrived:
        ours = ours + a.astype(F32)
    ours = lax.optimization_barrier(ours).astype(BF16)

    ours, split = lax.optimization_barrier((ours, split))
    devices = nz * ny * nx * nc
    rows = added(split)
    both = jnp.concatenate([jnp.broadcast_to(rows[None], (plane,) + rows.shape), ours], axis=2)
    both = lax.all_to_all(both, ("z", "y"), 0, 0)
    total = spread(added(both[:, :, width:]), ("z", "y", "x", "c"), devices)
    grad_w_out = both[:, :, :width].astype(F32).reshape(PAIR, width)
    grad_w, *vectors = unpack(total.reshape(plane, pairs, CHUNK, BLK))
    return (grad_u[None], grad_v[None], grad_w_out, grad_w, *vectors)


def solution(mesh):
    devices = mesh.devices.reshape(4, -1, *[mesh.devices.shape[1] // 2, 2])
    grid = Mesh(devices, ("z", "y", "x", "c"))
    big = P(("x", "c"), ("z", "y"), None)
    rows = P(("x", "c"), None)
    return jax.shard_map(
        functools.partial(on_device, sizes=devices.shape),
        mesh=grid,
        in_specs=(big, big, big, P(), P(), P(), P(), rows),
        out_specs=(big, big, rows, P(), P(), P(), P()),
        check_vma=False,
    )
```

```python
import functools

import jax
import jax.numpy as jnp
from jax import lax
from jax.experimental import pallas as pl
from jax.experimental.pallas import tpu as pltpu
from jax.sharding import Mesh, PartitionSpec as P

EPS = 1e-05
C0 = 0.7978845608028654
C1 = C0 * 0.044715
F32 = jnp.float32
BF16 = jnp.bfloat16
BLK = 128
PAIR = 256
SIDE = 16
PACK = 9 * BLK
ROOT = BLK**0.5


def tanh_of(a):
    a2 = a * a
    return jnp.tanh(a * (C0 + C1 * a2)), a2


def gelu(a):
    t, _ = tanh_of(a)
    return a * (0.5 + 0.5 * t)


def gelu_and_slope(a):
    t, a2 = tanh_of(a)
    half = 0.5 + 0.5 * t
    value = a * half
    return value, half + value * (1.0 - half) * (2.0 * C0 + (6.0 * C1) * a2)


def norm(gated):
    centre = gated - jnp.mean(gated, axis=-1, keepdims=True)
    inverse = lax.rsqrt(jnp.sum(centre * centre, axis=-1, keepdims=True) + BLK * EPS)
    return centre * inverse, inverse


def lower_of(a):
    row = lax.broadcasted_iota(jnp.int32, a.shape, 0)
    col = lax.broadcasted_iota(jnp.int32, a.shape, 1)
    return jnp.where(row >= col, a, jnp.zeros_like(a))


def upright(row):
    return jnp.broadcast_to(row, (BLK, BLK)).T


def columns(ref, at, first=0, count=None):
    count = ref.shape[0] if count is None else count
    return jnp.concatenate([ref[first + k, at] for k in range(count)], axis=1)


def scatter_columns(src, dst, sem):
    @pl.loop(0, dst.shape[0])
    def _(k):
        at = pl.ds(pl.multiple_of(k * BLK, BLK), BLK)
        pltpu.make_async_copy(src.at[:, at], dst.at[k], sem).start()


def await_all(dst, sem):
    pltpu.make_async_copy(dst, dst, sem).wait()


def cols_of(g):
    return slice(g * BLK, (g + 1) * BLK)


def forward_kernel(
    order, u_ref, v_ref, d_hbm, w_ref, bias_ref, gain_ref, shift_ref, out_ref, d_ref, go_ref, low_at, bias_at, sem
):
    blocks, length, _ = d_ref.shape
    turns = length // PAIR
    step = pl.program_id(0)
    last = pl.num_programs(0) - 1
    now, before = lax.rem(step, 2), lax.rem(step + 1, 2)
    part = blocks // turns

    def multiply(i):
        out_ref[0, :, i * part * BLK : (i + 1) * part * BLK] = jnp.dot(
            go_ref[before],
            columns(d_ref, slice(None), i * part, part),
            preferred_element_type=F32,
        ).astype(out_ref.dtype)

    def gate(i):
        rows = [slice(i * PAIR + h * BLK, i * PAIR + (h + 1) * BLK) for h in range(2)]
        for g in range(2):
            gain, shift = ROOT * gain_ref[0, g : g + 1], shift_ref[0, g : g + 1]
            normed = []
            for at in rows:
                scaled, _ = norm(gelu(v_ref[at, cols_of(g)].astype(F32)))
                normed.append((scaled * gain + shift).astype(BF16))
            mixed = jnp.dot(
                low_at[g], jnp.concatenate(normed, axis=1), preferred_element_type=F32
            )
            for h, at in enumerate(rows):
                upper = gelu(u_ref[at, cols_of(g)].astype(F32))
                gated_out = (upper * (mixed[:, cols_of(h)] + bias_at[g])).astype(BF16)
                go_ref[now, cols_of(g), at] = gated_out.T

    @pl.when(step == 0)
    def _():
        scatter_columns(d_hbm, d_ref, sem)

    for g in range(2):
        bias_at[g] = upright(bias_ref[0, g : g + 1])
        low_at[g] = lower_of(w_ref[0, g].astype(F32)).astype(BF16)

    @pl.when(step == 0)
    def _():
        for i in range(turns):
            gate(i)
        await_all(d_ref, sem)

    @pl.when((step > 0) & (step < last))
    def _():
        for i in range(turns):
            multiply(i)
            gate(i)

    @pl.when(step == last)
    def _():
        for i in range(turns):
            multiply(i)


def forward(here, theirs, u, v, d, mix, bias, gain, shift):
    length, width = u.shape
    n = width // PAIR // 2
    last = n - 1
    pair_at = lambda j, o: 2 * jnp.minimum(j, last) + (1 - o[1] if theirs else o[1])
    cur = lambda j, o: (0, pair_at(j, o))
    par = lambda j, o: (pair_at(j, o), 0, 0)
    return pl.pallas_call(
        forward_kernel,
        grid_spec=pltpu.PrefetchScalarGridSpec(
            num_scalar_prefetch=1,
            grid=(n + 1,),
            in_specs=[
                pl.BlockSpec((length, PAIR), cur),
                pl.BlockSpec((length, PAIR), cur),
                pl.BlockSpec(memory_space=pl.ANY),
                pl.BlockSpec((1, 2, BLK, BLK), lambda j, o: (pair_at(j, o), 0, 0, 0)),
                pl.BlockSpec((1, 2, BLK), par),
                pl.BlockSpec((1, 2, BLK), par),
                pl.BlockSpec((1, 2, BLK), par),
            ],
            out_specs=pl.BlockSpec((1, PAIR, width), lambda j, o: (jnp.maximum(j - 1, 0), 0, 0)),
            scratch_shapes=[
                pltpu.VMEM((width // BLK, length, BLK), BF16),
                pltpu.VMEM((2, PAIR, length), BF16),
                pltpu.VMEM((2, BLK, BLK), BF16),
                pltpu.VMEM((2, BLK, BLK), F32),
                pltpu.SemaphoreType.DMA,
            ],
        ),
        out_shape=jax.ShapeDtypeStruct((n, PAIR, width), BF16),
        cost_estimate=pl.CostEstimate(
            flops=2 * n * PAIR * length * (width + BLK) * 2,
            bytes_accessed=length * width * 2 + n * PAIR * (4 * length + 2 * width),
            transcendentals=2 * n * PAIR * length,
        ),
        name="fwd",
    )(here, u, v, d, mix, bias, gain, shift)


def backward_kernel(
    pieces, order, u_ref, v_ref, d_hbm, mix_ref, bias_ref, gain_ref, shift_ref, *rest
):
    count = len(pieces)
    w_hbm = rest[:count]
    gu_ref, gv_ref, pack_ref = rest[-14:-11]
    d_ref, w_ref, cot_ref, low_at, turned_at, bias_at, b_acc, g_acc, s_acc, m_acc, sems = rest[-11:]
    turns = u_ref.shape[0] // PAIR
    step = pl.program_id(0)
    last = pl.num_programs(0) - 1

    def landing(k):
        slot, start, size = pieces[k]
        return w_ref.at[slot, :, pl.ds(start, size)]

    def cotangent(i, slot):
        return lax.dot_general(
            columns(d_ref, slice(i * PAIR, (i + 1) * PAIR)),
            columns(w_ref.at[slot], slice(None)),
            (((1,), (1,)), ((), ())),
            preferred_element_type=F32,
        )

    @pl.when(step == 0)
    def _():
        for k in range(count):
            if pieces[k][0] == 0:
                scatter_columns(w_hbm[k], landing(k), sems.at[k])
        scatter_columns(d_hbm, d_ref, sems.at[count])
        for k in range(count):
            if pieces[k][0] > 0:
                scatter_columns(w_hbm[k], landing(k), sems.at[k])
        for k in range(count):
            if pieces[k][0] == 0:
                await_all(landing(k), sems.at[k])
        await_all(d_ref, sems.at[count])
        cot_ref[0] = cotangent(0, 0)

    for k in range(count):
        if pieces[k][0] > 0:
            @pl.when(step == pieces[k][0] - 1)
            def _(k=k):
                await_all(landing(k), sems.at[k])

    for g in range(2):
        lower = lower_of(mix_ref[0, g].astype(F32))
        low_at[g] = lower.astype(BF16)
        turned_at[g] = lower.T.astype(BF16)
        bias_at[g] = upright(bias_ref[0, g : g + 1])
    b_acc[...] = jnp.zeros_like(b_acc)
    g_acc[...] = jnp.zeros_like(g_acc)
    s_acc[...] = jnp.zeros_like(s_acc)
    m_acc[...] = jnp.zeros_like(m_acc)
    for i in range(turns):
        if i + 1 < turns:
            cot_ref[(i + 1) % 2] = cotangent(i + 1, step)
        else:
            cot_ref[0] = cotangent(0, jnp.minimum(step + 1, last))
        for g in range(2):
            gain, shift = ROOT * gain_ref[0, g : g + 1], shift_ref[0, g : g + 1]
            rows = [slice(i * PAIR + h * BLK, i * PAIR + (h + 1) * BLK) for h in range(2)]
            kept, normed = [], []
            for at in rows:
                gated, slope = gelu_and_slope(v_ref[at, cols_of(g)].astype(F32))
                scaled, inverse = norm(gated)
                kept.append((scaled, inverse * slope))
                normed.append((scaled * gain + shift).astype(BF16))
            normed = jnp.concatenate(normed, axis=1)
            mixed = jnp.dot(low_at[g], normed, preferred_element_type=F32)
            d_mixed_b = []
            for h, at in enumerate(rows):
                upper, slope = gelu_and_slope(u_ref[at, cols_of(g)].astype(F32))
                cot = cot_ref[i % 2, h * BLK : (h + 1) * BLK, cols_of(g)]
                d_mixed = cot * upper
                d_mixed_b.append(d_mixed.astype(BF16))
                b_acc[g] += d_mixed
                gu_ref[at, cols_of(g)] = (
                    cot * slope * (mixed[:, cols_of(h)] + bias_at[g])
                ).astype(BF16)
            d_mixed_b = jnp.concatenate(d_mixed_b, axis=1)
            m_acc[g] += lax.dot_general(
                d_mixed_b, normed, (((1,), (1,)), ((), ())), preferred_element_type=F32
            )
            d_normed = jnp.dot(turned_at[g], d_mixed_b, preferred_element_type=F32)
            for h, at in enumerate(rows):
                scaled, scale = kept[h]
                dn = d_normed[:, cols_of(h)]
                weighted = dn * scaled
                g_acc[g] += jnp.sum(weighted.reshape(BLK // 8, 8, BLK), axis=0)
                s_acc[g] += jnp.sum(dn.reshape(BLK // 8, 8, BLK), axis=0)
                e = dn * gain
                mean_e = jnp.mean(e, axis=-1, keepdims=True)
                sum_es = jnp.sum(weighted * gain, axis=-1, keepdims=True)
                gv_ref[at, cols_of(g)] = (scale * (e - mean_e - scaled * sum_es)).astype(BF16)

    extra = []
    for g in range(2):
        extra.append(jnp.sum(b_acc[g].T, axis=0, keepdims=True))
        extra.append(ROOT * jnp.sum(g_acc[g], axis=0, keepdims=True))
        extra.append(jnp.sum(s_acc[g], axis=0, keepdims=True))
    row = lax.broadcasted_iota(jnp.int32, (BLK, BLK), 0)
    col = lax.broadcasted_iota(jnp.int32, (BLK, BLK), 1)
    extra.append(jnp.sum(jnp.where(row == col, m_acc[1], 0.0), axis=0, keepdims=True))
    both = jnp.where(row >= col, m_acc[0], m_acc[1].T)
    while len(extra) < SIDE:
        extra.append(jnp.zeros((1, BLK), F32))
    tiles = [both[k * SIDE : (k + 1) * SIDE] for k in range(BLK // SIDE)]
    tiles.append(jnp.concatenate(extra, axis=0))
    pack_ref[0] = jnp.concatenate(tiles, axis=1).astype(BF16)


def unpack_kernel(x_ref, gw_ref, gb_ref, gg_ref, gs_ref):
    pairs = x_ref.shape[0]
    row = lax.broadcasted_iota(jnp.int32, (BLK, BLK), 0)
    col = lax.broadcasted_iota(jnp.int32, (BLK, BLK), 1)

    @pl.loop(0, pairs)
    def _(pair):
        x = x_ref[pair].astype(F32)
        both = jnp.concatenate([x[:, cols_of(k)] for k in range(BLK // SIDE)], axis=0)
        vector = lambda k: x[k : k + 1, cols_of(BLK // SIDE)]
        gw_ref[2 * pair] = jnp.where(row >= col, both, 0.0)
        gw_ref[2 * pair + 1] = jnp.where(
            row > col, both.T, jnp.where(row == col, vector(6), 0.0)
        )
        for g in range(2):
            at = pl.ds(2 * pair + g, 1)
            gb_ref[at] = vector(3 * g)
            gg_ref[at] = vector(3 * g + 1)
            gs_ref[at] = vector(3 * g + 2)


def unpack(total):
    pairs = total.shape[0]
    row = jax.ShapeDtypeStruct((2 * pairs, BLK), F32)
    return pl.pallas_call(
        unpack_kernel,
        out_shape=[jax.ShapeDtypeStruct((2 * pairs, BLK, BLK), F32), row, row, row],
        cost_estimate=pl.CostEstimate(flops=10**6, bytes_accessed=10**6, transcendentals=0),
        name="unpack",
    )(total)


def join_kernel(a_hbm, b_hbm, out_hbm, a_ref, b_ref, out_ref, sems):
    count = a_hbm.shape[0]
    hbm = (a_hbm, b_hbm, out_hbm)
    vmem = (a_ref, b_ref, out_ref)
    read = lambda s, k: pltpu.make_async_copy(hbm[s].at[k], vmem[s].at[k], sems.at[s, k])
    write = lambda k: pltpu.make_async_copy(out_ref.at[k], out_hbm.at[k], sems.at[2, k])

    for k in range(count):
        read(0, k).start()
        read(1, k).start()

    @pl.loop(0, count)
    def _(k):
        read(0, k).wait()
        read(1, k).wait()
        out_ref[k] = (a_ref[k].astype(F32) + b_ref[k].astype(F32)).astype(BF16)
        write(k).start()

    for k in range(count):
        write(k).wait()


def join(a, b):
    n, rows, width = a.shape
    parts = (4 * n, rows // 4, width)
    hbm = pl.BlockSpec(memory_space=pl.ANY)
    return pl.pallas_call(
        join_kernel,
        in_specs=[hbm, hbm],
        out_specs=hbm,
        out_shape=jax.ShapeDtypeStruct(parts, BF16),
        scratch_shapes=[pltpu.VMEM(parts, BF16)] * 3 + [pltpu.SemaphoreType.DMA((3, 4 * n))],
        cost_estimate=pl.CostEstimate(
            flops=a.size, bytes_accessed=6 * a.size, transcendentals=0
        ),
        name="join",
    )(a.reshape(parts), b.reshape(parts)).reshape(a.shape)


def backward(here, weights, u, v, d, mix, bias, gain, shift):
    length, width = u.shape
    n = pairs = width // PAIR
    half = n // 2

    def pair_at(j, o):
        core = jnp.where(j < half, 1 - o[1], o[1])
        return lax.rem(o[0] + o[2 + lax.rem(j, half)], half) * 2 + core

    pieces = tuple((slot, start, w.shape[0]) for slot, start, w in weights)
    cur = lambda j, o: (0, pair_at(j, o))
    par = lambda j, o: (pair_at(j, o), 0, 0)
    mat = pl.BlockSpec((1, 2, BLK, BLK), lambda j, o: (pair_at(j, o), 0, 0, 0))
    tile = pl.BlockSpec((length, PAIR), cur)
    vec = pl.BlockSpec((1, 2, BLK), par)
    hbm = pl.BlockSpec(memory_space=pl.ANY)
    shapes = [
        jax.ShapeDtypeStruct((length, width), BF16),
        jax.ShapeDtypeStruct((length, width), BF16),
        jax.ShapeDtypeStruct((pairs, SIDE, PACK), BF16),
    ]
    return pl.pallas_call(
        functools.partial(backward_kernel, pieces),
        grid_spec=pltpu.PrefetchScalarGridSpec(
            num_scalar_prefetch=1,
            grid=(n,),
            in_specs=[
                tile,
                tile,
                hbm,
                mat,
                vec,
                vec,
                vec,
                *[hbm] * len(weights),
            ],
            out_specs=[
                tile,
                tile,
                pl.BlockSpec((1, SIDE, PACK), lambda j, o: (j, 0, 0)),
            ],
            scratch_shapes=[
                pltpu.VMEM((width // BLK, length, BLK), BF16),
                pltpu.VMEM((n, width // BLK, PAIR, BLK), BF16),
                pltpu.VMEM((2, PAIR, PAIR), F32),
                pltpu.VMEM((2, BLK, BLK), BF16),
                pltpu.VMEM((2, BLK, BLK), BF16),
                pltpu.VMEM((2, BLK, BLK), F32),
                pltpu.VMEM((2, BLK, BLK), F32),
                pltpu.VMEM((2, 8, BLK), F32),
                pltpu.VMEM((2, 8, BLK), F32),
                pltpu.VMEM((2, BLK, BLK), F32),
                pltpu.SemaphoreType.DMA((len(weights) + 1,)),
            ],
        ),
        out_shape=shapes,
        cost_estimate=pl.CostEstimate(
            flops=2 * n * PAIR * length * (width + 3 * BLK) * 2,
            bytes_accessed=length * width * 2 + n * PAIR * (8 * length + 2 * width),
            transcendentals=3 * n * PAIR * length,
        ),
        name="bwd",
    )(here, u, v, d, mix, bias, gain, shift, *[w for _, _, w in weights])


def hop(a, axis, size, by):
    return lax.ppermute(a, axis, [(i, (i + by) % size) for i in range(size)])


def added(a):
    return lax.optimization_barrier(jnp.sum(a.astype(F32), axis=0)).astype(BF16)


def spread(a, axes, count):
    return lax.all_to_all(jnp.broadcast_to(a[None], (count,) + a.shape), axes, 0, 0)


def on_device(u_pre, v_pre, d_out, w_mix, mix_bias, norm_gain, norm_shift, w_out, sizes=None):
    return everything(
        u_pre, v_pre, d_out, w_mix, mix_bias, norm_gain, norm_shift, w_out, sizes
    )


def everything(u_pre, v_pre, d_out, w_mix, mix_bias, norm_gain, norm_shift, w_out, sizes):
    nz, ny, nx, nc = sizes
    plane = nz * ny
    u, v, d = u_pre[0], v_pre[0], d_out[0]
    _, width = u.shape
    groups = w_mix.shape[0]
    pairs = groups // 2
    x, c = lax.axis_index("x"), lax.axis_index("c")
    hops = jnp.array([0, nx - 1, 1, 2], jnp.int32)
    here = jnp.concatenate([jnp.stack([x, c]).astype(jnp.int32), hops])

    swap = lambda a: hop(a, "c", nc, 1)
    half = w_out.shape[0] // 2
    own = swap(w_out)
    left = hop(w_out, "x", nx, 1)
    right = hop(w_out, "x", nx, -1)
    far0 = hop(left[:half], "x", nx, 1)
    far1 = hop(right[half:], "x", nx, -1)
    near = [swap(left), swap(right)]
    far = [swap(far0), swap(far1)]

    mix = w_mix.reshape(pairs, 2, BLK, BLK)
    bias = mix_bias.reshape(pairs, 2, BLK)
    gain = norm_gain.reshape(pairs, 2, BLK)
    shift = norm_shift.reshape(pairs, 2, BLK)

    common = (u, v, d, mix, bias, gain, shift)
    theirs = forward(here, True, *common)
    ours = forward(here, False, *common)
    traded = swap(theirs)
    joined = join(ours, traded)
    split = lax.all_to_all(joined.reshape(nx * plane, PAIR // plane, width), ("x", "z", "y"), 0, 0)

    weights = [
        (0, 0, own),
        (1, 0, near[0]),
        (2, 0, near[1]),
        (3, 0, far[0]),
        (3, half, far[1]),
        (4, 0, w_out),
        (5, 0, left),
        (6, 0, right),
        (7, 0, far0),
        (7, half, far1),
    ]
    grad_u, grad_v, packed = backward(here, weights, *common)

    mine = packed[nx:].astype(F32) + swap(packed[:nx]).astype(F32)
    mine = lax.optimization_barrier(mine).astype(BF16)
    arrived = [hop(mine[1], "x", nx, -1), hop(mine[2], "x", nx, 1), hop(mine[3], "x", nx, 2)]
    ours = mine[0].astype(F32)
    for a in arrived:
        ours = ours + a.astype(F32)
    ours = lax.optimization_barrier(ours).astype(BF16)

    ours, split = lax.optimization_barrier((ours, split))
    both = jnp.concatenate([added(split), ours], axis=1)
    both = spread(both, ("z", "y"), plane)
    total = spread(added(both[:, :, width:]), ("x", "c"), nx * nc)
    grad_w_out = both[:, :, :width].astype(F32).reshape(PAIR, width)
    grad_w, *vectors = unpack(total)
    return (grad_u[None], grad_v[None], grad_w_out, grad_w, *vectors)


def solution(mesh):
    devices = mesh.devices.reshape(4, -1, *[mesh.devices.shape[1] // 2, 2])
    grid = Mesh(devices, ("z", "y", "x", "c"))
    big = P(("x", "c"), ("z", "y"), None)
    rows = P(("x", "c"), None)
    return jax.shard_map(
        functools.partial(on_device, sizes=devices.shape),
        mesh=grid,
        in_specs=(big, big, big, P(), P(), P(), P(), rows),
        out_specs=(big, big, rows, P(), P(), P(), P()),
        check_vma=False,
    )
```

```python
import functools

import jax
import jax.numpy as jnp
from jax import lax
from jax.experimental import pallas as pl
from jax.experimental.pallas import tpu as pltpu
from jax.sharding import Mesh, PartitionSpec as P

EPS = 1e-05
C0 = 0.7978845608028654
C1 = C0 * 0.044715
F32 = jnp.float32
BF16 = jnp.bfloat16
BLK = 128
PAIR = 256
SIDE = 16
PACK = 9 * BLK
ROOT = BLK**0.5


def tanh_of(a):
    a2 = a * a
    return jnp.tanh(a * (C0 + C1 * a2)), a2


def gelu(a):
    t, _ = tanh_of(a)
    return a * (0.5 + 0.5 * t)


def gelu_and_slope(a):
    t, a2 = tanh_of(a)
    half = 0.5 + 0.5 * t
    value = a * half
    return value, half + value * (1.0 - half) * (2.0 * C0 + (6.0 * C1) * a2)


def norm(gated):
    centre = gated - jnp.mean(gated, axis=-1, keepdims=True)
    inverse = lax.rsqrt(jnp.sum(centre * centre, axis=-1, keepdims=True) + BLK * EPS)
    return centre * inverse, inverse


def lower_of(a):
    row = lax.broadcasted_iota(jnp.int32, a.shape, 0)
    col = lax.broadcasted_iota(jnp.int32, a.shape, 1)
    return jnp.where(row >= col, a, jnp.zeros_like(a))


def upright(row):
    return jnp.broadcast_to(row, (BLK, BLK)).T


def columns(ref, at, first=0, count=None):
    count = ref.shape[0] if count is None else count
    return jnp.concatenate([ref[first + k, at] for k in range(count)], axis=1)


def scatter_columns(src, dst, sem):
    @pl.loop(0, dst.shape[0])
    def _(k):
        at = pl.ds(pl.multiple_of(k * BLK, BLK), BLK)
        pltpu.make_async_copy(src.at[:, at], dst.at[k], sem).start()


def await_all(dst, sem):
    pltpu.make_async_copy(dst, dst, sem).wait()


def cols_of(g):
    return slice(g * BLK, (g + 1) * BLK)


def forward_kernel(
    order, u_ref, v_ref, d_hbm, w_ref, bias_ref, gain_ref, shift_ref, out_ref, d_ref, go_ref, low_at, bias_at, sem
):
    blocks, length, _ = d_ref.shape
    turns = length // PAIR
    step = pl.program_id(0)
    last = pl.num_programs(0) - 1
    now, before = lax.rem(step, 2), lax.rem(step + 1, 2)
    part = blocks // turns

    def multiply(i):
        out_ref[0, :, i * part * BLK : (i + 1) * part * BLK] = jnp.dot(
            go_ref[before],
            columns(d_ref, slice(None), i * part, part),
            preferred_element_type=F32,
        ).astype(out_ref.dtype)

    def gate(i):
        rows = [slice(i * PAIR + h * BLK, i * PAIR + (h + 1) * BLK) for h in range(2)]
        for g in range(2):
            gain, shift = ROOT * gain_ref[0, g : g + 1], shift_ref[0, g : g + 1]
            normed = []
            for at in rows:
                scaled, _ = norm(gelu(v_ref[at, cols_of(g)].astype(F32)))
                normed.append((scaled * gain + shift).astype(BF16))
            mixed = jnp.dot(
                low_at[g], jnp.concatenate(normed, axis=1), preferred_element_type=F32
            )
            for h, at in enumerate(rows):
                upper = gelu(u_ref[at, cols_of(g)].astype(F32))
                gated_out = (upper * (mixed[:, cols_of(h)] + bias_at[g])).astype(BF16)
                go_ref[now, cols_of(g), at] = gated_out.T

    @pl.when(step == 0)
    def _():
        scatter_columns(d_hbm, d_ref, sem)

    for g in range(2):
        bias_at[g] = upright(bias_ref[0, g : g + 1])
        low_at[g] = lower_of(w_ref[0, g].astype(F32)).astype(BF16)

    @pl.when(step == 0)
    def _():
        for i in range(turns):
            gate(i)
        await_all(d_ref, sem)

    @pl.when((step > 0) & (step < last))
    def _():
        for i in range(turns):
            multiply(i)
            gate(i)

    @pl.when(step == last)
    def _():
        for i in range(turns):
            multiply(i)


def forward(here, theirs, u, v, d, mix, bias, gain, shift):
    length, width = u.shape
    n = width // PAIR // 2
    last = n - 1
    pair_at = lambda j, o: 2 * jnp.minimum(j, last) + (1 - o[1] if theirs else o[1])
    cur = lambda j, o: (0, pair_at(j, o))
    par = lambda j, o: (pair_at(j, o), 0, 0)
    return pl.pallas_call(
        forward_kernel,
        grid_spec=pltpu.PrefetchScalarGridSpec(
            num_scalar_prefetch=1,
            grid=(n + 1,),
            in_specs=[
                pl.BlockSpec((length, PAIR), cur),
                pl.BlockSpec((length, PAIR), cur),
                pl.BlockSpec(memory_space=pl.ANY),
                pl.BlockSpec((1, 2, BLK, BLK), lambda j, o: (pair_at(j, o), 0, 0, 0)),
                pl.BlockSpec((1, 2, BLK), par),
                pl.BlockSpec((1, 2, BLK), par),
                pl.BlockSpec((1, 2, BLK), par),
            ],
            out_specs=pl.BlockSpec((1, PAIR, width), lambda j, o: (jnp.maximum(j - 1, 0), 0, 0)),
            scratch_shapes=[
                pltpu.VMEM((width // BLK, length, BLK), BF16),
                pltpu.VMEM((2, PAIR, length), BF16),
                pltpu.VMEM((2, BLK, BLK), BF16),
                pltpu.VMEM((2, BLK, BLK), F32),
                pltpu.SemaphoreType.DMA,
            ],
        ),
        out_shape=jax.ShapeDtypeStruct((n, PAIR, width), BF16),
        cost_estimate=pl.CostEstimate(
            flops=2 * n * PAIR * length * (width + BLK) * 2,
            bytes_accessed=length * width * 2 + n * PAIR * (4 * length + 2 * width),
            transcendentals=2 * n * PAIR * length,
        ),
        name="fwd",
    )(here, u, v, d, mix, bias, gain, shift)


def backward_kernel(
    pieces, order, u_ref, v_ref, d_hbm, mix_ref, bias_ref, gain_ref, shift_ref, *rest
):
    count = len(pieces)
    w_hbm = rest[:count]
    gu_ref, gv_ref, pack_ref = rest[-14:-11]
    d_ref, w_ref, cot_ref, low_at, turned_at, bias_at, b_acc, g_acc, s_acc, m_acc, sems = rest[-11:]
    turns = u_ref.shape[0] // PAIR
    step = pl.program_id(0)
    last = pl.num_programs(0) - 1

    def landing(k):
        slot, start, size = pieces[k]
        return w_ref.at[slot, :, pl.ds(start, size)]

    def cotangent(i, slot):
        return lax.dot_general(
            columns(d_ref, slice(i * PAIR, (i + 1) * PAIR)),
            columns(w_ref.at[slot], slice(None)),
            (((1,), (1,)), ((), ())),
            preferred_element_type=F32,
        )

    @pl.when(step == 0)
    def _():
        for k in range(count):
            if pieces[k][0] == 0:
                scatter_columns(w_hbm[k], landing(k), sems.at[k])
        scatter_columns(d_hbm, d_ref, sems.at[count])
        for k in range(count):
            if pieces[k][0] > 0:
                scatter_columns(w_hbm[k], landing(k), sems.at[k])
        for k in range(count):
            if pieces[k][0] == 0:
                await_all(landing(k), sems.at[k])
        await_all(d_ref, sems.at[count])
        cot_ref[0] = cotangent(0, 0)

    for k in range(count):
        if pieces[k][0] > 0:
            @pl.when(step == pieces[k][0] - 1)
            def _(k=k):
                await_all(landing(k), sems.at[k])

    for g in range(2):
        lower = lower_of(mix_ref[0, g].astype(F32))
        low_at[g] = lower.astype(BF16)
        turned_at[g] = lower.T.astype(BF16)
        bias_at[g] = upright(bias_ref[0, g : g + 1])
    b_acc[...] = jnp.zeros_like(b_acc)
    g_acc[...] = jnp.zeros_like(g_acc)
    s_acc[...] = jnp.zeros_like(s_acc)
    m_acc[...] = jnp.zeros_like(m_acc)
    for i in range(turns):
        if i + 1 < turns:
            cot_ref[(i + 1) % 2] = cotangent(i + 1, step)
        else:
            cot_ref[0] = cotangent(0, jnp.minimum(step + 1, last))
        for g in range(2):
            gain, shift = ROOT * gain_ref[0, g : g + 1], shift_ref[0, g : g + 1]
            rows = [slice(i * PAIR + h * BLK, i * PAIR + (h + 1) * BLK) for h in range(2)]
            kept, normed = [], []
            for at in rows:
                gated, slope = gelu_and_slope(v_ref[at, cols_of(g)].astype(F32))
                scaled, inverse = norm(gated)
                kept.append((scaled, inverse * slope))
                normed.append((scaled * gain + shift).astype(BF16))
            normed = jnp.concatenate(normed, axis=1)
            mixed = jnp.dot(low_at[g], normed, preferred_element_type=F32)
            d_mixed_b = []
            for h, at in enumerate(rows):
                upper, slope = gelu_and_slope(u_ref[at, cols_of(g)].astype(F32))
                cot = cot_ref[i % 2, h * BLK : (h + 1) * BLK, cols_of(g)]
                d_mixed = cot * upper
                d_mixed_b.append(d_mixed.astype(BF16))
                b_acc[g] += d_mixed
                gu_ref[at, cols_of(g)] = (
                    cot * slope * (mixed[:, cols_of(h)] + bias_at[g])
                ).astype(BF16)
            d_mixed_b = jnp.concatenate(d_mixed_b, axis=1)
            m_acc[g] += lax.dot_general(
                d_mixed_b, normed, (((1,), (1,)), ((), ())), preferred_element_type=F32
            )
            d_normed = jnp.dot(turned_at[g], d_mixed_b, preferred_element_type=F32)
            for h, at in enumerate(rows):
                scaled, scale = kept[h]
                dn = d_normed[:, cols_of(h)]
                weighted = dn * scaled
                g_acc[g] += jnp.sum(weighted.reshape(BLK // 8, 8, BLK), axis=0)
                s_acc[g] += jnp.sum(dn.reshape(BLK // 8, 8, BLK), axis=0)
                e = dn * gain
                mean_e = jnp.mean(e, axis=-1, keepdims=True)
                sum_es = jnp.sum(weighted * gain, axis=-1, keepdims=True)
                gv_ref[at, cols_of(g)] = (scale * (e - mean_e - scaled * sum_es)).astype(BF16)

    extra = []
    for g in range(2):
        extra.append(jnp.sum(b_acc[g].T, axis=0, keepdims=True))
        extra.append(ROOT * jnp.sum(g_acc[g], axis=0, keepdims=True))
        extra.append(jnp.sum(s_acc[g], axis=0, keepdims=True))
    row = lax.broadcasted_iota(jnp.int32, (BLK, BLK), 0)
    col = lax.broadcasted_iota(jnp.int32, (BLK, BLK), 1)
    extra.append(jnp.sum(jnp.where(row == col, m_acc[1], 0.0), axis=0, keepdims=True))
    both = jnp.where(row >= col, m_acc[0], m_acc[1].T)
    while len(extra) < SIDE:
        extra.append(jnp.zeros((1, BLK), F32))
    tiles = [both[k * SIDE : (k + 1) * SIDE] for k in range(BLK // SIDE)]
    tiles.append(jnp.concatenate(extra, axis=0))
    pack_ref[0] = jnp.concatenate(tiles, axis=1).astype(BF16)


def unpack_kernel(here, mine_ref, theirs_ref, gw_ref, gb_ref, gg_ref, gs_ref):
    count = mine_ref.shape[0]
    row = lax.broadcasted_iota(jnp.int32, (BLK, BLK), 0)
    col = lax.broadcasted_iota(jnp.int32, (BLK, BLK), 1)

    @pl.loop(0, count)
    def _(k):
        first = 2 * lax.rem(here[0] - k + count, count)
        for ref, core in ((mine_ref, here[1]), (theirs_ref, 1 - here[1])):
            pair = first + core
            x = ref[k].astype(F32)
            both = jnp.concatenate([x[:, cols_of(j)] for j in range(BLK // SIDE)], axis=0)
            vector = lambda j: x[j : j + 1, cols_of(BLK // SIDE)]
            gw_ref[2 * pair] = jnp.where(row >= col, both, 0.0)
            gw_ref[2 * pair + 1] = jnp.where(
                row > col, both.T, jnp.where(row == col, vector(6), 0.0)
            )
            for g in range(2):
                at = pl.ds(2 * pair + g, 1)
                gb_ref[at] = vector(3 * g)
                gg_ref[at] = vector(3 * g + 1)
                gs_ref[at] = vector(3 * g + 2)


def unpack(here, mine, theirs):
    groups = 4 * mine.shape[0]
    row = jax.ShapeDtypeStruct((groups, BLK), F32)
    vmem = pl.BlockSpec(memory_space=pltpu.VMEM)
    return pl.pallas_call(
        unpack_kernel,
        in_specs=[pl.BlockSpec(memory_space=pltpu.SMEM), vmem, vmem],
        out_specs=[vmem] * 4,
        out_shape=[jax.ShapeDtypeStruct((groups, BLK, BLK), F32), row, row, row],
        cost_estimate=pl.CostEstimate(flops=10**6, bytes_accessed=10**6, transcendentals=0),
        name="unpack",
    )(here, mine, theirs)


def join_kernel(a_hbm, b_hbm, out_hbm, a_ref, b_ref, out_ref, sems):
    count = a_hbm.shape[0]
    hbm = (a_hbm, b_hbm, out_hbm)
    vmem = (a_ref, b_ref, out_ref)
    read = lambda s, k: pltpu.make_async_copy(hbm[s].at[k], vmem[s].at[k], sems.at[s, k])
    write = lambda k: pltpu.make_async_copy(out_ref.at[k], out_hbm.at[k], sems.at[2, k])

    for k in range(count):
        read(0, k).start()
        read(1, k).start()

    @pl.loop(0, count)
    def _(k):
        read(0, k).wait()
        read(1, k).wait()
        out_ref[k] = (a_ref[k].astype(F32) + b_ref[k].astype(F32)).astype(BF16)
        write(k).start()

    for k in range(count):
        write(k).wait()


def join(a, b):
    n, rows, width = a.shape
    parts = (4 * n, rows // 4, width)
    hbm = pl.BlockSpec(memory_space=pl.ANY)
    return pl.pallas_call(
        join_kernel,
        in_specs=[hbm, hbm],
        out_specs=hbm,
        out_shape=jax.ShapeDtypeStruct(parts, BF16),
        scratch_shapes=[pltpu.VMEM(parts, BF16)] * 3 + [pltpu.SemaphoreType.DMA((3, 4 * n))],
        cost_estimate=pl.CostEstimate(
            flops=a.size, bytes_accessed=6 * a.size, transcendentals=0
        ),
        name="join",
    )(a.reshape(parts), b.reshape(parts)).reshape(a.shape)


def backward(here, weights, u, v, d, mix, bias, gain, shift):
    length, width = u.shape
    n = pairs = width // PAIR
    half = n // 2

    def pair_at(j, o):
        core = jnp.where(j < half, 1 - o[1], o[1])
        return lax.rem(o[0] + lax.rem(j, half), half) * 2 + core

    pieces = tuple((slot, start, w.shape[0]) for slot, start, w in weights)
    cur = lambda j, o: (0, pair_at(j, o))
    par = lambda j, o: (pair_at(j, o), 0, 0)
    mat = pl.BlockSpec((1, 2, BLK, BLK), lambda j, o: (pair_at(j, o), 0, 0, 0))
    tile = pl.BlockSpec((length, PAIR), cur)
    vec = pl.BlockSpec((1, 2, BLK), par)
    hbm = pl.BlockSpec(memory_space=pl.ANY)
    shapes = [
        jax.ShapeDtypeStruct((length, width), BF16),
        jax.ShapeDtypeStruct((length, width), BF16),
        jax.ShapeDtypeStruct((pairs, SIDE, PACK), BF16),
    ]
    return pl.pallas_call(
        functools.partial(backward_kernel, pieces),
        grid_spec=pltpu.PrefetchScalarGridSpec(
            num_scalar_prefetch=1,
            grid=(n,),
            in_specs=[
                tile,
                tile,
                hbm,
                mat,
                vec,
                vec,
                vec,
                *[hbm] * len(weights),
            ],
            out_specs=[
                tile,
                tile,
                pl.BlockSpec((1, SIDE, PACK), lambda j, o: (j, 0, 0)),
            ],
            scratch_shapes=[
                pltpu.VMEM((width // BLK, length, BLK), BF16),
                pltpu.VMEM((n, width // BLK, PAIR, BLK), BF16),
                pltpu.VMEM((2, PAIR, PAIR), F32),
                pltpu.VMEM((2, BLK, BLK), BF16),
                pltpu.VMEM((2, BLK, BLK), BF16),
                pltpu.VMEM((2, BLK, BLK), F32),
                pltpu.VMEM((2, BLK, BLK), F32),
                pltpu.VMEM((2, 8, BLK), F32),
                pltpu.VMEM((2, 8, BLK), F32),
                pltpu.VMEM((2, BLK, BLK), F32),
                pltpu.SemaphoreType.DMA((len(weights) + 1,)),
            ],
        ),
        out_shape=shapes,
        cost_estimate=pl.CostEstimate(
            flops=2 * n * PAIR * length * (width + 3 * BLK) * 2,
            bytes_accessed=length * width * 2 + n * PAIR * (8 * length + 2 * width),
            transcendentals=3 * n * PAIR * length,
        ),
        name="bwd",
    )(here, u, v, d, mix, bias, gain, shift, *[w for _, _, w in weights])


def hop(a, axis, size, by):
    return lax.ppermute(a, axis, [(i, (i + by) % size) for i in range(size)])


def total_of(parts):
    a, b, c, d = [p.astype(F32) for p in parts]
    return lax.optimization_barrier((a + c) + (b + d)).astype(BF16)


def added(a):
    return lax.optimization_barrier(jnp.sum(a.astype(F32), axis=0)).astype(BF16)


def spread(a, axes, count):
    return lax.all_to_all(jnp.broadcast_to(a[None], (count,) + a.shape), axes, 0, 0)


def on_device(u_pre, v_pre, d_out, w_mix, mix_bias, norm_gain, norm_shift, w_out, sizes=None):
    return everything(
        u_pre, v_pre, d_out, w_mix, mix_bias, norm_gain, norm_shift, w_out, sizes
    )


def everything(u_pre, v_pre, d_out, w_mix, mix_bias, norm_gain, norm_shift, w_out, sizes):
    nz, ny, nx, nc = sizes
    plane = nz * ny
    u, v, d = u_pre[0], v_pre[0], d_out[0]
    _, width = u.shape
    groups = w_mix.shape[0]
    pairs = groups // 2
    x, c = lax.axis_index("x"), lax.axis_index("c")
    here = jnp.stack([x, c]).astype(jnp.int32)

    swap = lambda a: hop(a, "c", nc, 1)
    half = w_out.shape[0] // 2
    own = swap(w_out)
    left = hop(w_out, "x", nx, 1)
    right = hop(w_out, "x", nx, -1)
    far0 = hop(left[:half], "x", nx, 1)
    far1 = hop(right[half:], "x", nx, -1)
    near = [swap(left), swap(right)]
    far = [swap(far0), swap(far1)]

    mix = w_mix.reshape(pairs, 2, BLK, BLK)
    bias = mix_bias.reshape(pairs, 2, BLK)
    gain = norm_gain.reshape(pairs, 2, BLK)
    shift = norm_shift.reshape(pairs, 2, BLK)

    common = (u, v, d, mix, bias, gain, shift)
    theirs = forward(here, True, *common)
    ours = forward(here, False, *common)
    traded = swap(theirs)
    joined = join(ours, traded)
    split = lax.all_to_all(joined.reshape(nx * plane, PAIR // plane, width), ("x", "z", "y"), 0, 0)

    weights = [
        (0, 0, own),
        (1, 0, near[1]),
        (2, 0, far[0]),
        (2, half, far[1]),
        (3, 0, near[0]),
        (4, 0, w_out),
        (5, 0, right),
        (6, 0, far0),
        (6, half, far1),
        (7, 0, left),
    ]
    grad_u, grad_v, packed = backward(here, weights, *common)

    mine = packed[nx:].astype(F32) + swap(packed[:nx]).astype(F32)
    mine = lax.optimization_barrier(mine).astype(BF16)
    arrived = [hop(mine[k], "x", nx, k) for k in range(1, nx)]
    ours = total_of([mine[0]] + arrived)
    for axis, size in (("y", ny), ("z", nz)):
        arrived = [hop(ours, axis, size, k) for k in range(1, size)]
        ours = total_of([ours] + arrived)
    rows = added(split)
    gathered = spread(rows, ("z", "y"), plane)
    ours = jnp.stack([ours] + [hop(ours, "x", nx, k) for k in range(1, nx)])
    others = swap(ours)
    grad_w, *vectors = unpack(here, ours, others)
    grad_w_out = gathered.reshape(PAIR, width).astype(F32)
    return (grad_u[None], grad_v[None], grad_w_out, grad_w, *vectors)


def solution(mesh):
    devices = mesh.devices.reshape(4, -1, *[mesh.devices.shape[1] // 2, 2])
    grid = Mesh(devices, ("z", "y", "x", "c"))
    big = P(("x", "c"), ("z", "y"), None)
    rows = P(("x", "c"), None)
    return jax.shard_map(
        functools.partial(on_device, sizes=devices.shape),
        mesh=grid,
        in_specs=(big, big, big, P(), P(), P(), P(), rows),
        out_specs=(big, big, rows, P(), P(), P(), P()),
        check_vma=False,
    )
```

```python
import functools

import jax
import jax.numpy as jnp
from jax import lax
from jax.experimental import pallas as pl
from jax.experimental.pallas import tpu as pltpu
from jax.sharding import Mesh, PartitionSpec as P

EPS = 1e-05
C0 = 0.7978845608028654
C1 = C0 * 0.044715
F32 = jnp.float32
BF16 = jnp.bfloat16
BLK = 128
PAIR = 256
SIDE = 16
PACK = 9 * BLK
ROOT = BLK**0.5


def tanh_of(a):
    a2 = a * a
    return jnp.tanh(a * (C0 + C1 * a2)), a2


def gelu(a):
    t, _ = tanh_of(a)
    return a * (0.5 + 0.5 * t)


def gelu_and_slope(a):
    t, a2 = tanh_of(a)
    half = 0.5 + 0.5 * t
    value = a * half
    return value, half + value * (1.0 - half) * (2.0 * C0 + (6.0 * C1) * a2)


def norm(gated):
    centre = gated - jnp.mean(gated, axis=-1, keepdims=True)
    inverse = lax.rsqrt(jnp.sum(centre * centre, axis=-1, keepdims=True) + BLK * EPS)
    return centre * inverse, inverse


def lower_of(a):
    row = lax.broadcasted_iota(jnp.int32, a.shape, 0)
    col = lax.broadcasted_iota(jnp.int32, a.shape, 1)
    return jnp.where(row >= col, a, jnp.zeros_like(a))


def upright(row):
    return jnp.broadcast_to(row, (BLK, BLK)).T


def columns(ref, at, first=0, count=None):
    count = ref.shape[0] if count is None else count
    return jnp.concatenate([ref[first + k, at] for k in range(count)], axis=1)


def scatter_columns(src, dst, sem):
    @pl.loop(0, dst.shape[0])
    def _(k):
        at = pl.ds(pl.multiple_of(k * BLK, BLK), BLK)
        pltpu.make_async_copy(src.at[:, at], dst.at[k], sem).start()


def await_all(dst, sem):
    pltpu.make_async_copy(dst, dst, sem).wait()


def cols_of(g):
    return slice(g * BLK, (g + 1) * BLK)


def forward_kernel(
    order, u_ref, v_ref, d_hbm, w_ref, bias_ref, gain_ref, shift_ref, out_ref, d_ref, go_ref, low_at, bias_at, sem
):
    blocks, length, _ = d_ref.shape
    turns = length // PAIR
    step = pl.program_id(0)
    last = pl.num_programs(0) - 1
    now, before = lax.rem(step, 2), lax.rem(step + 1, 2)
    part = blocks // turns

    def multiply(i):
        out_ref[0, :, i * part * BLK : (i + 1) * part * BLK] = jnp.dot(
            go_ref[before],
            columns(d_ref, slice(None), i * part, part),
            preferred_element_type=F32,
        ).astype(out_ref.dtype)

    def gate(i):
        rows = [slice(i * PAIR + h * BLK, i * PAIR + (h + 1) * BLK) for h in range(2)]
        for g in range(2):
            gain, shift = ROOT * gain_ref[0, g : g + 1], shift_ref[0, g : g + 1]
            normed = []
            for at in rows:
                scaled, _ = norm(gelu(v_ref[at, cols_of(g)].astype(F32)))
                normed.append((scaled * gain + shift).astype(BF16))
            mixed = jnp.dot(
                low_at[g], jnp.concatenate(normed, axis=1), preferred_element_type=F32
            )
            for h, at in enumerate(rows):
                upper = gelu(u_ref[at, cols_of(g)].astype(F32))
                gated_out = (upper * (mixed[:, cols_of(h)] + bias_at[g])).astype(BF16)
                go_ref[now, cols_of(g), at] = gated_out.T

    @pl.when(step == 0)
    def _():
        scatter_columns(d_hbm, d_ref, sem)

    for g in range(2):
        bias_at[g] = upright(bias_ref[0, g : g + 1])
        low_at[g] = lower_of(w_ref[0, g].astype(F32)).astype(BF16)

    @pl.when(step == 0)
    def _():
        for i in range(turns):
            gate(i)
        await_all(d_ref, sem)

    @pl.when((step > 0) & (step < last))
    def _():
        for i in range(turns):
            multiply(i)
            gate(i)

    @pl.when(step == last)
    def _():
        for i in range(turns):
            multiply(i)


def forward(here, theirs, u, v, d, mix, bias, gain, shift):
    length, width = u.shape
    n = width // PAIR // 2
    last = n - 1
    pair_at = lambda j, o: 2 * jnp.minimum(j, last) + (1 - o[1] if theirs else o[1])
    cur = lambda j, o: (0, pair_at(j, o))
    par = lambda j, o: (pair_at(j, o), 0, 0)
    return pl.pallas_call(
        forward_kernel,
        grid_spec=pltpu.PrefetchScalarGridSpec(
            num_scalar_prefetch=1,
            grid=(n + 1,),
            in_specs=[
                pl.BlockSpec((length, PAIR), cur),
                pl.BlockSpec((length, PAIR), cur),
                pl.BlockSpec(memory_space=pl.ANY),
                pl.BlockSpec((1, 2, BLK, BLK), lambda j, o: (pair_at(j, o), 0, 0, 0)),
                pl.BlockSpec((1, 2, BLK), par),
                pl.BlockSpec((1, 2, BLK), par),
                pl.BlockSpec((1, 2, BLK), par),
            ],
            out_specs=pl.BlockSpec((1, PAIR, width), lambda j, o: (jnp.maximum(j - 1, 0), 0, 0)),
            scratch_shapes=[
                pltpu.VMEM((width // BLK, length, BLK), BF16),
                pltpu.VMEM((2, PAIR, length), BF16),
                pltpu.VMEM((2, BLK, BLK), BF16),
                pltpu.VMEM((2, BLK, BLK), F32),
                pltpu.SemaphoreType.DMA,
            ],
        ),
        out_shape=jax.ShapeDtypeStruct((n, PAIR, width), BF16),
        cost_estimate=pl.CostEstimate(
            flops=2 * n * PAIR * length * (width + BLK) * 2,
            bytes_accessed=length * width * 2 + n * PAIR * (4 * length + 2 * width),
            transcendentals=2 * n * PAIR * length,
        ),
        name="fwd",
    )(here, u, v, d, mix, bias, gain, shift)


def backward_kernel(
    pieces, order, u_ref, v_ref, d_hbm, mix_ref, bias_ref, gain_ref, shift_ref, *rest
):
    count = len(pieces)
    w_hbm = rest[:count]
    gu_ref, gv_ref, pack_ref = rest[-14:-11]
    d_ref, w_ref, cot_ref, low_at, turned_at, bias_at, b_acc, g_acc, s_acc, m_acc, sems = rest[-11:]
    turns = u_ref.shape[0] // PAIR
    step = pl.program_id(0)
    last = pl.num_programs(0) - 1

    def landing(k):
        slot, start, size = pieces[k]
        return w_ref.at[slot, :, pl.ds(start, size)]

    def cotangent(i, slot):
        return lax.dot_general(
            columns(d_ref, slice(i * PAIR, (i + 1) * PAIR)),
            columns(w_ref.at[slot], slice(None)),
            (((1,), (1,)), ((), ())),
            preferred_element_type=F32,
        )

    @pl.when(step == 0)
    def _():
        for k in range(count):
            if pieces[k][0] == 0:
                scatter_columns(w_hbm[k], landing(k), sems.at[k])
        scatter_columns(d_hbm, d_ref, sems.at[count])
        for k in range(count):
            if pieces[k][0] > 0:
                scatter_columns(w_hbm[k], landing(k), sems.at[k])
        for k in range(count):
            if pieces[k][0] == 0:
                await_all(landing(k), sems.at[k])
        await_all(d_ref, sems.at[count])
        cot_ref[0] = cotangent(0, 0)

    for k in range(count):
        if pieces[k][0] > 0:
            @pl.when(step == pieces[k][0] - 1)
            def _(k=k):
                await_all(landing(k), sems.at[k])

    for g in range(2):
        lower = lower_of(mix_ref[0, g].astype(F32))
        low_at[g] = lower.astype(BF16)
        turned_at[g] = lower.T.astype(BF16)
        bias_at[g] = upright(bias_ref[0, g : g + 1])
    b_acc[...] = jnp.zeros_like(b_acc)
    g_acc[...] = jnp.zeros_like(g_acc)
    s_acc[...] = jnp.zeros_like(s_acc)
    m_acc[...] = jnp.zeros_like(m_acc)
    for i in range(turns):
        if i + 1 < turns:
            cot_ref[(i + 1) % 2] = cotangent(i + 1, step)
        else:
            cot_ref[0] = cotangent(0, jnp.minimum(step + 1, last))
        for g in range(2):
            gain, shift = ROOT * gain_ref[0, g : g + 1], shift_ref[0, g : g + 1]
            rows = [slice(i * PAIR + h * BLK, i * PAIR + (h + 1) * BLK) for h in range(2)]
            kept, normed = [], []
            for at in rows:
                gated, slope = gelu_and_slope(v_ref[at, cols_of(g)].astype(F32))
                scaled, inverse = norm(gated)
                kept.append((scaled, inverse * slope))
                normed.append((scaled * gain + shift).astype(BF16))
            normed = jnp.concatenate(normed, axis=1)
            mixed = jnp.dot(low_at[g], normed, preferred_element_type=F32)
            d_mixed_b = []
            for h, at in enumerate(rows):
                upper, slope = gelu_and_slope(u_ref[at, cols_of(g)].astype(F32))
                cot = cot_ref[i % 2, h * BLK : (h + 1) * BLK, cols_of(g)]
                d_mixed = cot * upper
                d_mixed_b.append(d_mixed.astype(BF16))
                b_acc[g] += d_mixed
                gu_ref[at, cols_of(g)] = (
                    cot * slope * (mixed[:, cols_of(h)] + bias_at[g])
                ).astype(BF16)
            d_mixed_b = jnp.concatenate(d_mixed_b, axis=1)
            m_acc[g] += lax.dot_general(
                d_mixed_b, normed, (((1,), (1,)), ((), ())), preferred_element_type=F32
            )
            d_normed = jnp.dot(turned_at[g], d_mixed_b, preferred_element_type=F32)
            for h, at in enumerate(rows):
                scaled, scale = kept[h]
                dn = d_normed[:, cols_of(h)]
                weighted = dn * scaled
                g_acc[g] += jnp.sum(weighted.reshape(BLK // 8, 8, BLK), axis=0)
                s_acc[g] += jnp.sum(dn.reshape(BLK // 8, 8, BLK), axis=0)
                e = dn * gain
                mean_e = jnp.mean(e, axis=-1, keepdims=True)
                sum_es = jnp.sum(weighted * gain, axis=-1, keepdims=True)
                gv_ref[at, cols_of(g)] = (scale * (e - mean_e - scaled * sum_es)).astype(BF16)

    extra = []
    for g in range(2):
        extra.append(jnp.sum(b_acc[g].T, axis=0, keepdims=True))
        extra.append(ROOT * jnp.sum(g_acc[g], axis=0, keepdims=True))
        extra.append(jnp.sum(s_acc[g], axis=0, keepdims=True))
    row = lax.broadcasted_iota(jnp.int32, (BLK, BLK), 0)
    col = lax.broadcasted_iota(jnp.int32, (BLK, BLK), 1)
    extra.append(jnp.sum(jnp.where(row == col, m_acc[1], 0.0), axis=0, keepdims=True))
    both = jnp.where(row >= col, m_acc[0], m_acc[1].T)
    while len(extra) < SIDE:
        extra.append(jnp.zeros((1, BLK), F32))
    tiles = [both[k * SIDE : (k + 1) * SIDE] for k in range(BLK // SIDE)]
    tiles.append(jnp.concatenate(extra, axis=0))
    pack_ref[0] = jnp.concatenate(tiles, axis=1).astype(BF16)


def unpack_kernel(here, mine_ref, theirs_ref, gw_ref, gb_ref, gg_ref, gs_ref):
    count = mine_ref.shape[0]
    row = lax.broadcasted_iota(jnp.int32, (BLK, BLK), 0)
    col = lax.broadcasted_iota(jnp.int32, (BLK, BLK), 1)

    @pl.loop(0, count)
    def _(k):
        first = 2 * lax.rem(here[0] - k + count, count)
        for ref, core in ((mine_ref, here[1]), (theirs_ref, 1 - here[1])):
            pair = first + core
            x = ref[k].astype(F32)
            both = jnp.concatenate([x[:, cols_of(j)] for j in range(BLK // SIDE)], axis=0)
            vector = lambda j: x[j : j + 1, cols_of(BLK // SIDE)]
            gw_ref[2 * pair] = jnp.where(row >= col, both, 0.0)
            gw_ref[2 * pair + 1] = jnp.where(
                row > col, both.T, jnp.where(row == col, vector(6), 0.0)
            )
            for g in range(2):
                at = pl.ds(2 * pair + g, 1)
                gb_ref[at] = vector(3 * g)
                gg_ref[at] = vector(3 * g + 1)
                gs_ref[at] = vector(3 * g + 2)


def unpack(here, mine, theirs):
    groups = 4 * mine.shape[0]
    row = jax.ShapeDtypeStruct((groups, BLK), F32)
    vmem = pl.BlockSpec(memory_space=pltpu.VMEM)
    return pl.pallas_call(
        unpack_kernel,
        in_specs=[pl.BlockSpec(memory_space=pltpu.SMEM), vmem, vmem],
        out_specs=[vmem] * 4,
        out_shape=[jax.ShapeDtypeStruct((groups, BLK, BLK), F32), row, row, row],
        cost_estimate=pl.CostEstimate(flops=10**6, bytes_accessed=10**6, transcendentals=0),
        name="unpack",
    )(here, mine, theirs)


def join_kernel(a_hbm, b_hbm, out_hbm, a_ref, b_ref, out_ref, sems):
    count = a_hbm.shape[0]
    hbm = (a_hbm, b_hbm, out_hbm)
    vmem = (a_ref, b_ref, out_ref)
    read = lambda s, k: pltpu.make_async_copy(hbm[s].at[k], vmem[s].at[k], sems.at[s, k])
    write = lambda k: pltpu.make_async_copy(out_ref.at[k], out_hbm.at[k], sems.at[2, k])

    for k in range(count):
        read(0, k).start()
        read(1, k).start()

    @pl.loop(0, count)
    def _(k):
        read(0, k).wait()
        read(1, k).wait()
        out_ref[k] = (a_ref[k].astype(F32) + b_ref[k].astype(F32)).astype(BF16)
        write(k).start()

    for k in range(count):
        write(k).wait()


def join(a, b):
    n, rows, width = a.shape
    parts = (4 * n, rows // 4, width)
    hbm = pl.BlockSpec(memory_space=pl.ANY)
    return pl.pallas_call(
        join_kernel,
        in_specs=[hbm, hbm],
        out_specs=hbm,
        out_shape=jax.ShapeDtypeStruct(parts, BF16),
        scratch_shapes=[pltpu.VMEM(parts, BF16)] * 3 + [pltpu.SemaphoreType.DMA((3, 4 * n))],
        cost_estimate=pl.CostEstimate(
            flops=a.size, bytes_accessed=6 * a.size, transcendentals=0
        ),
        name="join",
    )(a.reshape(parts), b.reshape(parts)).reshape(a.shape)


def backward(here, weights, u, v, d, mix, bias, gain, shift):
    length, width = u.shape
    n = pairs = width // PAIR
    half = n // 2

    def pair_at(j, o):
        core = jnp.where(j < half, 1 - o[1], o[1])
        return lax.rem(o[0] + lax.rem(j, half), half) * 2 + core

    pieces = tuple((slot, start, w.shape[0]) for slot, start, w in weights)
    cur = lambda j, o: (0, pair_at(j, o))
    par = lambda j, o: (pair_at(j, o), 0, 0)
    mat = pl.BlockSpec((1, 2, BLK, BLK), lambda j, o: (pair_at(j, o), 0, 0, 0))
    tile = pl.BlockSpec((length, PAIR), cur)
    vec = pl.BlockSpec((1, 2, BLK), par)
    hbm = pl.BlockSpec(memory_space=pl.ANY)
    shapes = [
        jax.ShapeDtypeStruct((length, width), BF16),
        jax.ShapeDtypeStruct((length, width), BF16),
        jax.ShapeDtypeStruct((pairs, SIDE, PACK), BF16),
    ]
    return pl.pallas_call(
        functools.partial(backward_kernel, pieces),
        grid_spec=pltpu.PrefetchScalarGridSpec(
            num_scalar_prefetch=1,
            grid=(n,),
            in_specs=[
                tile,
                tile,
                hbm,
                mat,
                vec,
                vec,
                vec,
                *[hbm] * len(weights),
            ],
            out_specs=[
                tile,
                tile,
                pl.BlockSpec((1, SIDE, PACK), lambda j, o: (j, 0, 0)),
            ],
            scratch_shapes=[
                pltpu.VMEM((width // BLK, length, BLK), BF16),
                pltpu.VMEM((n, width // BLK, PAIR, BLK), BF16),
                pltpu.VMEM((2, PAIR, PAIR), F32),
                pltpu.VMEM((2, BLK, BLK), BF16),
                pltpu.VMEM((2, BLK, BLK), BF16),
                pltpu.VMEM((2, BLK, BLK), F32),
                pltpu.VMEM((2, BLK, BLK), F32),
                pltpu.VMEM((2, 8, BLK), F32),
                pltpu.VMEM((2, 8, BLK), F32),
                pltpu.VMEM((2, BLK, BLK), F32),
                pltpu.SemaphoreType.DMA((len(weights) + 1,)),
            ],
        ),
        out_shape=shapes,
        cost_estimate=pl.CostEstimate(
            flops=2 * n * PAIR * length * (width + 3 * BLK) * 2,
            bytes_accessed=length * width * 2 + n * PAIR * (8 * length + 2 * width),
            transcendentals=3 * n * PAIR * length,
        ),
        name="bwd",
    )(here, u, v, d, mix, bias, gain, shift, *[w for _, _, w in weights])


def hop(a, axis, size, by):
    return lax.ppermute(a, axis, [(i, (i + by) % size) for i in range(size)])


def row_sum_kernel(x_hbm, out_hbm, x_ref, acc_ref, row_ref, in_sems, out_sems):
    count, each = x_ref.shape[:2]
    copies = out_hbm.shape[0]
    read = lambda k: pltpu.make_async_copy(
        x_hbm.at[pl.ds(k * each, each)], x_ref.at[k], in_sems.at[k]
    )
    write = lambda k: pltpu.make_async_copy(row_ref, out_hbm.at[k], out_sems.at[k])

    for k in range(count):
        read(k).start()
    acc_ref[...] = jnp.zeros_like(acc_ref)

    @pl.loop(0, count)
    def _(k):
        read(k).wait()
        total = x_ref[k, 0].astype(F32)
        for r in range(1, each):
            total = total + x_ref[k, r].astype(F32)
        acc_ref[...] += total

    row_ref[...] = acc_ref[...].astype(BF16)
    for k in range(copies):
        write(k).start()
    for k in range(copies):
        write(k).wait()


def row_sum(x, copies):
    n, rows, width = x.shape
    count = 16
    hbm = pl.BlockSpec(memory_space=pl.ANY)
    return pl.pallas_call(
        row_sum_kernel,
        in_specs=[hbm],
        out_specs=hbm,
        out_shape=jax.ShapeDtypeStruct((copies, rows, width), BF16),
        scratch_shapes=[
            pltpu.VMEM((count, n // count, rows, width), BF16),
            pltpu.VMEM((rows, width), F32),
            pltpu.VMEM((rows, width), BF16),
            pltpu.SemaphoreType.DMA((count,)),
            pltpu.SemaphoreType.DMA((copies,)),
        ],
        cost_estimate=pl.CostEstimate(flops=x.size, bytes_accessed=3 * x.size, transcendentals=0),
        name="row_sum",
    )(x)


def total_of(parts):
    a, b, c, d = [p.astype(F32) for p in parts]
    return lax.optimization_barrier((a + c) + (b + d)).astype(BF16)


def on_device(u_pre, v_pre, d_out, w_mix, mix_bias, norm_gain, norm_shift, w_out, sizes=None):
    return everything(
        u_pre, v_pre, d_out, w_mix, mix_bias, norm_gain, norm_shift, w_out, sizes
    )


def everything(u_pre, v_pre, d_out, w_mix, mix_bias, norm_gain, norm_shift, w_out, sizes):
    nz, ny, nx, nc = sizes
    plane = nz * ny
    u, v, d = u_pre[0], v_pre[0], d_out[0]
    _, width = u.shape
    groups = w_mix.shape[0]
    pairs = groups // 2
    x, c = lax.axis_index("x"), lax.axis_index("c")
    here = jnp.stack([x, c]).astype(jnp.int32)

    swap = lambda a: hop(a, "c", nc, 1)
    half = w_out.shape[0] // 2
    own = swap(w_out)
    left = hop(w_out, "x", nx, 1)
    right = hop(w_out, "x", nx, -1)
    far0 = hop(left[:half], "x", nx, 1)
    far1 = hop(right[half:], "x", nx, -1)
    near = [swap(left), swap(right)]
    far = [swap(far0), swap(far1)]

    mix = w_mix.reshape(pairs, 2, BLK, BLK)
    bias = mix_bias.reshape(pairs, 2, BLK)
    gain = norm_gain.reshape(pairs, 2, BLK)
    shift = norm_shift.reshape(pairs, 2, BLK)

    common = (u, v, d, mix, bias, gain, shift)
    theirs = forward(here, True, *common)
    ours = forward(here, False, *common)
    traded = swap(theirs)
    joined = join(ours, traded)
    split = lax.all_to_all(joined.reshape(nx * plane, PAIR // plane, width), ("x", "z", "y"), 0, 0)

    weights = [
        (0, 0, own),
        (1, 0, near[1]),
        (2, 0, far[0]),
        (2, half, far[1]),
        (3, 0, near[0]),
        (4, 0, w_out),
        (5, 0, right),
        (6, 0, far0),
        (6, half, far1),
        (7, 0, left),
    ]
    grad_u, grad_v, packed = backward(here, weights, *common)

    mine = packed[nx:].astype(F32) + swap(packed[:nx]).astype(F32)
    mine = lax.optimization_barrier(mine).astype(BF16)
    arrived = [hop(mine[k], "x", nx, k) for k in range(1, nx)]
    ours = total_of([mine[0]] + arrived)
    for axis, size in (("y", ny), ("z", nz)):
        arrived = [hop(ours, axis, size, k) for k in range(1, size)]
        ours = total_of([ours] + arrived)
    rows = row_sum(split, plane)
    gathered = lax.all_to_all(rows, ("z", "y"), 0, 0)
    ours = jnp.stack([ours] + [hop(ours, "x", nx, k) for k in range(1, nx)])
    others = swap(ours)
    grad_w, *vectors = unpack(here, ours, others)
    grad_w_out = gathered.reshape(PAIR, width).astype(F32)
    return (grad_u[None], grad_v[None], grad_w_out, grad_w, *vectors)


def solution(mesh):
    devices = mesh.devices.reshape(4, -1, *[mesh.devices.shape[1] // 2, 2])
    grid = Mesh(devices, ("z", "y", "x", "c"))
    big = P(("x", "c"), ("z", "y"), None)
    rows = P(("x", "c"), None)
    return jax.shard_map(
        functools.partial(on_device, sizes=devices.shape),
        mesh=grid,
        in_specs=(big, big, big, P(), P(), P(), P(), rows),
        out_specs=(big, big, rows, P(), P(), P(), P()),
        check_vma=False,
    )
```
